32 devices in a mesh: ep: 8 (over z, x), tp: 4 (over y, core).
Axes of the slice: x: 2, y: 2, z: 4, core: 2. Of those that a mesh axis runs over, the one named last changes fastest.
Arguments:
- tokens: bfloat16 [128, 2048], P('ep'), may hold values from -6 to 6
- attn_gain: float32 [2048], replicated, may hold values from 0.1 to 1.9
- query_weight: bfloat16 [2048, 2048], P('ep', 'tp'), may hold values from -0.125 to 0.125
- key_weight: bfloat16 [2048, 512], P('ep', 'tp'), may hold values from -0.125 to 0.125
- value_weight: bfloat16 [2048, 512], P('ep', 'tp'), may hold values from -0.125 to 0.125
- break_bias: float32 [16], P('tp'), may hold values from -14 to -8
- cache_keys: bfloat16 [128, 4, 1024, 128], P('ep', 'tp'), may hold values from -18 to 18
- cache_values: bfloat16 [128, 4, 1024, 128], P('ep', 'tp'), may hold values from -6 to 6
- lengths: int32 [128], P('ep'), may hold values from 1 to 1024, 65536 in all
- out_weight: bfloat16 [2048, 2048], P('tp', 'ep'), may hold values from -0.25 to 0.25
- ffn_gain: float32 [2048], replicated, may hold values from 0.1 to 1.9
- branch_gate: bfloat16 [2048], replicated, may hold values from -0.125 to 0.125
- dense_gate: bfloat16 [2048, 8192], P('tp', 'ep'), may hold values from -0.125 to 0.125
- dense_up: bfloat16 [2048, 8192], P('tp', 'ep'), may hold values from -0.125 to 0.125
- dense_down: bfloat16 [8192, 2048], P('ep', 'tp'), may hold values from -0.0625 to 0.0625
- route_ids: int32 [128, 4], P('ep'), may hold values from 0 to 7, all different within a row; in each aligned block of 16 rows (0 to 15, 16 to 31, ...) at most 16 rows name the same one
- route_weights: float32 [128, 4], P('ep'), may hold values from 0.1 to 1
- expert_gate: bfloat16 [8, 2048, 1024], P('ep', None, 'tp'), may hold values from -0.4375 to 0.4375
- expert_up: bfloat16 [8, 2048, 1024], P('ep', None, 'tp'), may hold values from -0.4375 to 0.4375
- expert_down: bfloat16 [8, 1024, 2048], P('ep', 'tp'), may hold values from -0.01953125 to 0.01953125
Outputs:
- layer_out: bfloat16 [128, 2048], P('ep', 'tp')
- new_keys: bfloat16 [128, 512], P('ep', 'tp')
- new_values: bfloat16 [128, 512], P('ep', 'tp')
The draws below stay inside these ranges and needn't reach their ends.
Inputs may be any that keep to these rules, and one draw needn't show every extreme that they name: `route_ids`: each row names 4 different experts. Among the rows of one device no expert is named more than 16 times, a bound that some block reaches. Sequence b's cache holds keys at positions below lengths[b]; some sequence fills its whole cache.
All inputs are finite; a program needn't handle non-finite values. No bound on the sum of `lengths` on one device may be relied on, other than what follows from the above.
Results may differ from the reference program's by a relative error of at most 0.011.
Values may be sent and summed in bfloat16 or wider, within the bound.
A program may use at most 64 MiB of HBM per device.

```python
import math
import jax
import jax.numpy as jnp
import numpy as np
from jax import lax

D = 2048
HEADS = 16
KV_HEADS = 4
HEAD_DIM = 128
DENSE = 8192
EXPERT_W = 1024
TOP_K = 4
SEQS = 16
CACHE_LEN = 1024
SEQUENCES = 128
EXPERTS = 8
CAP = 16
N_EP = 8


def levels(key, extent, split, smallest, high):
    def one(axis_at, shards_of):
        draws = jax.random.uniform(jax.random.fold_in(jax.random.fold_in(key, 6), axis_at), (shards_of,), jnp.float32, smallest / len(split), high / len(split))
        return jnp.repeat(jnp.exp(draws), extent[axis_at] // shards_of).reshape((-1,) + (1,) * (len(extent) - axis_at - 1))

    loudness = one(*split[0])
    for cut in split[1:]:
        loudness = loudness * one(*cut)
    return loudness


def split_up(count, total, most, slope):
    loads = [(1 << 20) // math.isqrt(standing ** slope) + 1 for standing in range(2, count + 1)]
    spare, counts = total - most - (count - 1), [1] * (count - 1)
    while spare > 0:
        candidates = [i for i in range(count - 1) if counts[i] < most]
        pool, budget = sum([loads[i] for i in candidates]), spare
        for i in candidates:
            extra = min(most - counts[i], max(1, budget * loads[i] // pool), spare)
            counts[i] = counts[i] + extra
            spare = spare - extra
    return np.array([most] + counts)


def uneven_parts(rng, amount, total, reach, slope):
    if amount == 2:
        one = jax.random.randint(rng, (), max(1, total - reach), min(reach, total - 1) + 1)
        return jnp.stack([one, total - one])
    tallies = jnp.asarray(split_up(amount, total, reach, slope), jnp.int32)
    twos = (amount - 1) // 2
    giver, taker = tallies[1:1 + 2 * twos:2], tallies[2:2 + 2 * twos:2]
    slack = jnp.minimum(giver - 1, reach - taker)
    moved = jax.random.randint(jax.random.fold_in(rng, 1), (twos,), 0, 1 << 20) % (slack + 1)
    tallies = tallies.at[1:1 + 2 * twos:2].set(giver - moved).at[2:2 + 2 * twos:2].set(taker + moved)
    return tallies[jax.random.permutation(jax.random.fold_in(rng, 2), amount)]


def assign_block(key, own, number, rows, amount, top, most, lean):
    order = jax.random.permutation(key, amount)
    heavy_load, usual = portions_of(amount, rows * top, most, lean, True), portions_of(amount, rows * top, most, lean, False)
    places = jnp.arange(amount)

    def named(sizes, rotation):
        used = int((sizes > 0).sum())
        fixed = max(1, used // 4)
        moved = fixed + (places - fixed + rotation * (used - fixed)) % max(1, amount - fixed)
        return jnp.zeros((amount,), jnp.int32).at[order[jnp.where(places < fixed, places, moved)]].set(jnp.asarray(sizes, jnp.int32))

    sizes = jnp.where(number % 4 == 0, named(heavy_load, number // 4), named(usual, number - number // 4 - 1))
    mixed = jax.random.permutation(jax.random.fold_in(own, 3), amount)
    donor, taker = mixed[0:amount // 2 * 2:2], mixed[1:amount // 2 * 2:2]
    room = jnp.minimum(sizes[donor] - 1, most - sizes[taker]) // 2
    room = jnp.where((donor == order[0]) | (taker == order[0]) | (sizes[taker] == 0), 0, jnp.maximum(room, 0))
    moved = jax.random.randint(jax.random.fold_in(own, 4), (amount // 2,), 0, 1 << 20) % (room + 1)
    sizes = sizes.at[donor].add(-moved).at[taker].add(moved)
    labels = jnp.searchsorted(jnp.cumsum(sizes), jnp.arange(rows * top), side="right").astype(jnp.int32)
    grid = labels.reshape(top, rows).T
    grid = grid[jax.random.permutation(jax.random.fold_in(own, 1), rows)]
    rotation = jax.random.randint(jax.random.fold_in(own, 2), (rows, 1), 0, top)
    return jnp.take_along_axis(grid, (jnp.arange(top)[None, :] + rotation) % top, axis=1)


def portions_of(number_of, total, limit, slope, full):
    weights = [(1 << 20) // math.isqrt(standing ** slope) + 1 for standing in range(1, number_of + 1)]
    largest = limit if full else min(limit, max(-(-total // number_of), total * weights[0] // sum(weights)))
    least = 1 if total - largest >= number_of - 1 else 0
    holding, spare = [largest] + [least] * (number_of - 1), total - largest - least * (number_of - 1)
    while spare > 0:
        candidates = [i for i in range(1, number_of) if holding[i] < largest] or [i for i in range(1, number_of) if holding[i] < limit]
        pool, budget = sum([weights[i] for i in candidates]), spare
        for i in candidates:
            addition = min(limit - holding[i], max(1, budget * weights[i] // pool), spare)
            holding[i] = holding[i] + addition
            spare = spare - addition
    return np.array(holding)


def normal_values(rng, shape, width, limit, pieces=(), held_as=jnp.bfloat16):
    entries = width * jax.random.normal(rng, shape, jnp.float32)
    if pieces:
        entries = entries * levels(rng, shape, pieces, -0.22, 0.18)
    return jnp.clip(entries, -limit, limit).astype(held_as)


def setup_inputs(seed: int = 0) -> dict:
    splits = jax.random.split(jax.random.key(seed), 21)
    tokens = normal_values(splits[0], (SEQUENCES, D), 1.0, 6.0, ((0, 8),))
    attn_gain = jnp.clip(1.0 + 0.18 * jax.random.normal(splits[1], (D,), jnp.float32), 0.1, 1.9)
    query_weight = normal_values(splits[2], (D, HEADS * HEAD_DIM), D ** -0.5, 0.125, ((0, 8), (1, 4)))
    key_weight = normal_values(splits[3], (D, KV_HEADS * HEAD_DIM), D ** -0.5, 0.125, ((0, 8), (1, 4)))
    value_weight = normal_values(splits[4], (D, KV_HEADS * HEAD_DIM), D ** -0.5, 0.125, ((0, 8), (1, 4)))
    break_bias = jnp.clip(-14.0 + 6.0 * jax.random.uniform(splits[5], (HEADS,), jnp.float32) ** levels(splits[5], (HEADS,), ((0, 4),), -0.2, 0.2), -14.0, -8.0)
    cache_keys = normal_values(splits[6], (SEQUENCES, KV_HEADS, CACHE_LEN, HEAD_DIM), 3.0, 18.0, ((0, 8), (1, 4)))
    cache_values = normal_values(splits[7], (SEQUENCES, KV_HEADS, CACHE_LEN, HEAD_DIM), 1.0, 6.0, ((0, 8), (1, 4)))
    lengths = uneven_parts(splits[8], SEQUENCES, SEQUENCES * CACHE_LEN // 2, CACHE_LEN, 2).astype(jnp.int32)
    out_weight = normal_values(splits[9], (HEADS * HEAD_DIM, D), (HEADS * HEAD_DIM // 4) ** -0.5, 0.25, ((0, 4), (1, 8)))
    ffn_gain = jnp.clip(1.0 + 0.18 * jax.random.normal(splits[10], (D,), jnp.float32), 0.1, 1.9)
    branch_gate = normal_values(splits[11], (D,), D ** -0.5, 0.125)
    dense_gate = normal_values(splits[12], (D, DENSE), D ** -0.5, 0.125, ((0, 4), (1, 8)))
    dense_up = normal_values(splits[13], (D, DENSE), D ** -0.5, 0.125, ((0, 4), (1, 8)))
    dense_down = normal_values(splits[14], (DENSE, D), DENSE ** -0.5, 0.0625, ((0, 8), (1, 4)))
    route_ids_keys = jax.random.split(jax.random.fold_in(splits[15], 1), SEQUENCES // SEQS)
    route_ids_turns = jax.random.permutation(jax.random.fold_in(splits[15], 3), SEQUENCES // SEQS)
    route_ids = jax.vmap(lambda own, number: assign_block(jax.random.fold_in(splits[15], 2), own, number, SEQS, EXPERTS, TOP_K, CAP, 2))(route_ids_keys, route_ids_turns).reshape((SEQUENCES, TOP_K))
    route_weights = jnp.clip(jnp.exp(math.log(1.0) - 2.3025851 * jax.random.uniform(splits[16], (SEQUENCES, TOP_K), jnp.float32) ** levels(splits[16], (SEQUENCES, TOP_K), ((0, 8),), -0.2, 0.2)), 0.1, 1.0)
    expert_gate = normal_values(splits[17], (EXPERTS, D, EXPERT_W), (D // 12) ** -0.5, 0.4375, ((0, 8), (2, 4)))
    expert_up = normal_values(splits[18], (EXPERTS, D, EXPERT_W), (D // 12) ** -0.5, 0.4375, ((0, 8), (2, 4)))
    expert_down = normal_values(splits[19], (EXPERTS, EXPERT_W, D), (EXPERT_W * 80) ** -0.5, 0.01953125, ((0, 8), (1, 4)))
    return {"tokens": tokens, "attn_gain": attn_gain, "query_weight": query_weight, "key_weight": key_weight, "value_weight": value_weight, "break_bias": break_bias, "cache_keys": cache_keys, "cache_values": cache_values, "lengths": lengths, "out_weight": out_weight, "ffn_gain": ffn_gain, "branch_gate": branch_gate, "dense_gate": dense_gate, "dense_up": dense_up, "dense_down": dense_down, "route_ids": route_ids, "route_weights": route_weights, "expert_gate": expert_gate, "expert_up": expert_up, "expert_down": expert_down}


norm_eps = 1e-05
clamp_limit = 7.0
swish_alpha = 1.702

def rms_scale(values, gain):
    return values * lax.rsqrt(lax.optimization_barrier(jnp.mean(values * values, axis=-1, keepdims=True)) + norm_eps) * gain

def clamped_unit(gate_pre, up_pre):
    gate_c = jnp.minimum(gate_pre, clamp_limit)
    up_c = jnp.clip(up_pre, -clamp_limit, clamp_limit)
    return (up_c + 1.0) * gate_c * jax.nn.sigmoid(swish_alpha * gate_c)

def reference(tokens, attn_gain, query_weight, key_weight, value_weight, break_bias, cache_keys, cache_values, lengths, out_weight, ffn_gain, branch_gate, dense_gate, dense_up, dense_down, route_ids, route_weights, expert_gate, expert_up, expert_down):
    normed = rms_scale(tokens.astype(jnp.float32), attn_gain).astype(jnp.bfloat16)
    queries = jnp.dot(normed, query_weight, preferred_element_type=jnp.float32).astype(jnp.bfloat16)
    new_keys = jnp.dot(normed, key_weight, preferred_element_type=jnp.float32).astype(jnp.bfloat16)
    new_values = jnp.dot(normed, value_weight, preferred_element_type=jnp.float32).astype(jnp.bfloat16)
    group_size = HEADS // KV_HEADS
    query_heads = queries.reshape(SEQUENCES, KV_HEADS, group_size, HEAD_DIM)
    head_bias = break_bias.reshape(KV_HEADS, group_size)
    positions = jnp.arange(CACHE_LEN, dtype=jnp.int32)

    def one_sequence(packed):
        query_rows, key_rows, value_rows, length_now = packed
        scores = jnp.einsum('grd,gld->grl', query_rows.astype(jnp.float32), key_rows.astype(jnp.float32))
        scores = scores * HEAD_DIM ** (-0.5) + head_bias[:, :, None]
        inside = (positions < length_now)[None, None, :]
        log_keep = jnp.where(inside, jax.nn.log_sigmoid(-scores), 0.0)
        between = lax.cumsum(log_keep, axis=2, reverse=True) - log_keep
        weights = jnp.where(inside, jnp.exp(jax.nn.log_sigmoid(scores) + between), 0.0).astype(jnp.bfloat16)
        return jnp.einsum('grl,gld->grd', weights.astype(jnp.float32), value_rows.astype(jnp.float32)).astype(jnp.bfloat16)
    attended = lax.map(one_sequence, (query_heads, cache_keys, cache_values, lengths))
    attended = attended.reshape(SEQUENCES, HEADS * HEAD_DIM)
    mixed = jnp.dot(attended, out_weight, preferred_element_type=jnp.float32).astype(jnp.bfloat16)
    resid = tokens.astype(jnp.float32) + mixed.astype(jnp.float32)
    normed2 = rms_scale(resid, ffn_gain).astype(jnp.bfloat16)
    slot_count = N_EP * CAP
    token_ids = jnp.arange(SEQUENCES, dtype=jnp.int32)

    def per_expert(expert_sum, expert):
        route_hits = route_ids == expert
        chosen = jnp.any(route_hits, axis=1)
        scale_sum = lax.optimization_barrier(jnp.sum(jnp.where(route_hits, route_weights, 0.0), axis=1))
        place_index = jnp.cumsum(chosen.astype(jnp.int32)) - 1
        target = jnp.where(chosen, place_index, slot_count).astype(jnp.int32)
        row_index = jnp.zeros((slot_count + 1,), jnp.int32).at[target].set(token_ids)[:slot_count]
        picked_rows = normed2[row_index]
        gate_pre = jnp.dot(picked_rows, expert_gate[expert], preferred_element_type=jnp.float32)
        up_pre = jnp.dot(picked_rows, expert_up[expert], preferred_element_type=jnp.float32)
        activation = clamped_unit(gate_pre, up_pre).astype(jnp.bfloat16)
        expert_rows = jnp.dot(activation, expert_down[expert], preferred_element_type=jnp.float32).astype(jnp.bfloat16)
        slot_live = jnp.arange(slot_count, dtype=jnp.int32) < jnp.sum(chosen.astype(jnp.int32))
        row_scale = jnp.where(slot_live, scale_sum[row_index], 0.0)
        return (expert_sum.at[row_index].add(row_scale[:, None] * expert_rows.astype(jnp.float32)), None)
    expert_sum, unused_out = lax.scan(per_expert, jnp.zeros((SEQUENCES, D), jnp.float32), jnp.arange(EXPERTS, dtype=jnp.int32))
    gate_part = jnp.dot(normed2, dense_gate, preferred_element_type=jnp.float32)
    up_part = jnp.dot(normed2, dense_up, preferred_element_type=jnp.float32)
    hidden_units = (jax.nn.silu(gate_part) * up_part).astype(jnp.bfloat16)
    dense_out = jnp.dot(hidden_units, dense_down, preferred_element_type=jnp.float32)
    branch_scale = jax.nn.sigmoid(jnp.dot(normed2, branch_gate, preferred_element_type=jnp.float32))
    layer_out = (resid + expert_sum + branch_scale[:, None] * dense_out).astype(jnp.bfloat16)
    return (layer_out, new_keys, new_values)
```

```python
import functools
import jax
import jax.numpy as jnp
from jax import lax
from jax.experimental import pallas as pl
from jax.experimental.pallas import tpu as pltpu
from jax.sharding import PartitionSpec as P

norm_eps = 1e-05
clamp_limit = 7.0
swish_alpha = 1.702
f32, bf16 = jnp.float32, jnp.bfloat16
MESH = pl.DeviceIdType.MESH

INPUTS = (
    "tokens", "attn_gain", "query_weight", "key_weight", "value_weight", "break_bias",
    "cache_keys", "cache_values", "lengths", "out_weight", "ffn_gain", "branch_gate",
    "dense_gate", "dense_up", "dense_down", "route_ids", "route_weights", "expert_gate",
    "expert_up", "expert_down",
)
STREAMED = (
    "query_weight", "key_weight", "value_weight", "cache_keys", "cache_values", "out_weight",
    "dense_gate", "dense_up", "expert_gate", "expert_up", "expert_down", "dense_down",
)
SCALARS = ("break_bias", "lengths")


def dot(a, b):
    return jnp.dot(a, b, preferred_element_type=f32)


class Refs:
    pass


def layer_kernel(names, *refs):
    r = Refs()
    for name, ref in zip(names, refs):
        setattr(r, name, ref)
    E, T = lax.axis_size("ep"), lax.axis_size("tp")
    e, t = lax.axis_index("ep"), lax.axis_index("tp")
    S, D = r.tokens.shape
    N = E * S
    FE = r.query_weight.shape[0]
    QC = r.query_weight.shape[1]
    KC = r.key_weight.shape[1]
    CL, HD = r.cache_keys.shape[2], r.cache_keys.shape[3]
    G = QC // HD
    OC = r.out_weight.shape[1]
    GT = E // T
    DQ = D // T
    HQ = r.dense_gate.shape[1] // T
    L = r.expert_gate.shape[0]
    t1 = t + 1 - 2 * lax.rem(t, 2)
    t2 = lax.rem(t + 2, T)
    t3 = lax.rem(t1 + 2, T)

    local = {}
    for i, name in enumerate(STREAMED):
        copy = pltpu.make_async_copy(getattr(r, name), getattr(r, "v_" + name), r.load_sem.at[i])
        copy.start()
        local[name] = copy

    barrier = pltpu.get_barrier_semaphore()

    def greet_ep(step, carry):
        pl.semaphore_signal(
            barrier, inc=1, device_id=(lax.rem(e + step, E), t), device_id_type=MESH
        )
        return carry

    def greet_tp(step, carry):
        pl.semaphore_signal(
            barrier, inc=1, device_id=(e, lax.rem(t + step, T)), device_id_type=MESH
        )
        return carry

    lax.fori_loop(1, E, greet_ep, 0)
    lax.fori_loop(1, T, greet_tp, 0)

    def remote(src, dst, sems, at, where):
        send, recv = sems
        return pltpu.make_async_remote_copy(
            src_ref=src,
            dst_ref=dst,
            send_sem=send if at is None else send.at[at],
            recv_sem=recv if at is None else recv.at[at],
            device_id=where,
            device_id_type=MESH,
        )

    def ep_copy(src, dst, sems, step, per_peer=True):
        peer = lax.rem(e + step, E)
        return remote(src.at[peer] if per_peer else src, dst.at[e], sems, step - 1, (peer, t))

    def ep_loop(fn):
        def one(step, carry):
            fn(step)
            return carry

        lax.fori_loop(1, E, one, 0)

    def source(step):
        return lax.rem(e - step + E, E)

    sem_a = (r.a_send, r.a_recv)
    sem_q = (r.q_send, r.q_recv)
    sem_k = (r.k_send, r.k_recv)
    sem_r = (r.r_send, r.r_recv)
    sem_x = (r.x_send, r.x_recv)
    sem_c = (r.c_send, r.c_recv)
    sem_d = (r.d_send, r.d_recv)
    sem_e = (r.e_send, r.e_recv)
    sem_ey = (r.ey_send, r.ey_recv)
    sem_ec = (r.ec_send, r.ec_recv)
    sem_ez = (r.ez_send, r.ez_recv)
    sem_g = (r.g_send, r.g_recv)

    def one_of(at):
        return (r.one_send.at[at], r.one_recv.at[at])

    tokens = r.tokens[...].astype(f32)
    mean = jnp.mean(tokens * tokens, axis=-1, keepdims=True)
    normed = (tokens * lax.rsqrt(mean + norm_eps) * r.attn_gain[...]).astype(bf16)
    for p in range(E):
        r.st_a[p] = normed[:, p * FE : (p + 1) * FE]
        r.st_r[p] = r.tokens[:, p * FE : (p + 1) * FE]
    ids, route = r.route_ids[...], r.route_weights[...]

    def side(p, carry):
        for l in range(L):
            own = jnp.sum(jnp.where(ids == p * L + l, route, 0.0), axis=1, keepdims=True)
            r.st_x[p, l] = jnp.broadcast_to(own, (S, 128))
        return carry

    lax.fori_loop(0, E, side, 0)
    pl.semaphore_wait(barrier, E - 1 + T - 1)

    ep_loop(lambda step: ep_copy(r.st_a, r.got_a, sem_a, step).start())
    r.got_a[e] = r.st_a[e]
    r.got_r[e] = r.st_r[e]
    r.got_x[e] = r.st_x[e]
    local["query_weight"].wait()
    r.got_q[e] = dot(r.st_a[e], r.v_query_weight[...]).astype(bf16)

    def answer(step):
        ep_copy(r.st_a, r.got_a, sem_a, step).wait_recv()
        src = source(step)
        r.st_q[src] = dot(r.got_a[src], r.v_query_weight[...]).astype(bf16)
        remote(r.st_q.at[src], r.got_q.at[e], sem_q, step - 1, (src, t)).start()

    ep_loop(answer)
    local["key_weight"].wait()
    local["value_weight"].wait()
    rows = r.got_a[...].reshape(N, FE)
    r.st_k[:, :, :KC] = dot(rows, r.v_key_weight[...]).astype(bf16).reshape(E, S, KC)
    r.st_k[:, :, KC:] = dot(rows, r.v_value_weight[...]).astype(bf16).reshape(E, S, KC)
    r.got_k[e] = r.st_k[e]

    def background(step):
        ep_copy(r.st_r, r.got_r, sem_r, step).start()
        ep_copy(r.st_k, r.got_k, sem_k, step).start()
        ep_copy(r.st_x, r.got_x, sem_x, step).start()

    ep_loop(background)

    def answered(step):
        src = source(step)
        return remote(r.st_q.at[src], r.got_q.at[e], sem_q, step - 1, (src, t))

    ep_loop(lambda step: answered(step).wait_recv())

    def total_of(got):
        def add(j, total):
            return total + got[j].astype(f32)

        return lax.fori_loop(1, E, add, got[0].astype(f32))

    queries = total_of(r.got_q).astype(bf16).astype(f32)
    for h in range(G):
        r.q_rows[pl.ds(h, S, stride=G), :] = queries[:, h * HD : (h + 1) * HD]

    tile = 8
    per = tile // G
    low = lax.broadcasted_iota(jnp.int32, (tile, 1), 0)

    def pick(parts):
        out = parts[0]
        for i in range(1, per):
            out = jnp.where(low >= i * G, parts[i], out)
        return out

    local["cache_keys"].wait()
    for i in range(S // per):
        q8 = r.q_rows[i * tile : (i + 1) * tile, :].astype(bf16)
        parts = [
            lax.dot_general(
                q8, r.v_cache_keys[i * per + j, 0], (((1,), (1,)), ((), ())),
                preferred_element_type=f32,
            )
            for j in range(per)
        ]
        r.scores[i * tile : (i + 1) * tile, :] = pick(parts)
    heads = S * G
    row = lax.broadcasted_iota(jnp.int32, (heads, 1), 0)
    length = jnp.zeros((heads, 1), jnp.int32)
    bias = jnp.zeros((heads, 1), f32)
    for s in range(S):
        length = jnp.where(row // G == s, r.lengths[s], length)
    for h in range(G):
        bias = jnp.where(lax.rem(row, G) == h, r.break_bias[h], bias)
    W = min(256, CL)
    later = lax.broadcasted_iota(jnp.int32, (W, W), 0)
    later = later > lax.broadcasted_iota(jnp.int32, (W, W), 1)
    later = jnp.where(later, 1.0, 0.0).astype(bf16)
    after = jnp.zeros((heads, 1), f32)
    for c in reversed(range(CL // W)):
        z = r.scores[:, c * W : (c + 1) * W] * HD ** (-0.5) + bias
        inside = lax.broadcasted_iota(jnp.int32, (heads, W), 1) + c * W < length
        soft = jnp.log1p(jnp.exp(-jnp.abs(z)))
        keep = jnp.where(inside, -(jnp.maximum(z, 0.0) + soft), 0.0)
        high = keep.astype(bf16)
        rest = keep - high.astype(f32)
        middle = rest.astype(bf16)
        least = (rest - middle.astype(f32)).astype(bf16)
        between = dot(high, later) + dot(middle, later) + dot(least, later) + after
        after = after + jnp.sum(keep, axis=1, keepdims=True)
        chance = jnp.exp(jnp.minimum(z, 0.0) - soft + between)
        r.scores[:, c * W : (c + 1) * W] = jnp.where(inside, chance, 0.0)
    local["cache_values"].wait()
    for i in range(S // per):
        w8 = r.scores[i * tile : (i + 1) * tile, :].astype(bf16)
        parts = [dot(w8, r.v_cache_values[i * per + j, 0]) for j in range(per)]
        r.mixed_rows[i * tile : (i + 1) * tile, :] = pick(parts)
    for h in range(G):
        r.st_c[:, h * HD : (h + 1) * HD] = r.mixed_rows[pl.ds(h, S, stride=G), :].astype(bf16)

    def c_copy(step):
        return ep_copy(r.st_c, r.got_c, sem_c, step, per_peer=False)

    ep_loop(lambda step: c_copy(step).start())
    r.got_c[e] = r.st_c[...]
    ep_loop(lambda step: ep_copy(r.st_k, r.got_k, sem_k, step).wait_recv())
    new_rows = total_of(r.got_k).astype(bf16)
    r.new_keys[...] = new_rows[:, :KC]
    r.new_values[...] = new_rows[:, KC:]
    ep_loop(lambda step: ep_copy(r.st_r, r.got_r, sem_r, step).wait_recv())
    ep_loop(lambda step: ep_copy(r.st_x, r.got_x, sem_x, step).wait_recv())
    local["out_weight"].wait()
    ep_loop(lambda step: c_copy(step).wait_recv())
    part = dot(r.got_c[...].reshape(N, QC), r.v_out_weight[...]).astype(bf16)
    r.st_d[...] = part.reshape(T, GT, S, OC)

    def d_copy(step):
        peer = lax.rem(t + step, T)
        return remote(r.st_d.at[peer], r.got_d.at[t], sem_d, step - 1, (e, peer))

    for step in range(1, T):
        d_copy(step).start()
    r.got_d[t] = r.st_d[t]
    for step in range(1, T):
        d_copy(step).wait_recv()
    mixed = r.got_d[0].astype(f32)
    for j in range(1, T):
        mixed = mixed + r.got_d[j].astype(f32)
    mixed = mixed.astype(bf16).astype(f32)

    mine = pl.ds(t * GT, GT)
    r.st_e[...] = (r.got_r[mine].astype(f32) + mixed).astype(bf16)

    def e_copy(step):
        return remote(
            r.st_e, r.got_e.at[e, mine], sem_e, step - 1, (lax.rem(e + step, E), t)
        )

    ep_loop(lambda step: e_copy(step).start())
    r.got_e[e, mine] = r.st_e[...]

    def pass_on(src, group, sems, peer):
        block = r.got_e.at[src, pl.ds(group * GT, GT)]
        return remote(block, block, sems, src, (e, peer))

    remote(r.st_e, r.got_e.at[e, mine], sem_ey, e, (e, t2)).start()
    remote(r.st_e, r.got_e.at[e, mine], sem_ec, e, (e, t1)).start()

    def forward(step):
        e_copy(step).wait_recv()
        src = source(step)
        pass_on(src, t, sem_ey, t2).start()
        pass_on(src, t, sem_ec, t1).start()

    ep_loop(forward)

    def cross(step):
        src = source(step)
        pass_on(src, t, sem_ey, t2).wait_recv()
        pass_on(src, t2, sem_ez, t1).start()

    lax.fori_loop(0, E, lambda step, carry: (cross(step), carry)[1], 0)

    def landed(step):
        src = source(step)
        pass_on(src, t, sem_ec, t1).wait_recv()
        pass_on(src, t2, sem_ez, t1).wait_recv()

    lax.fori_loop(0, E, lambda step, carry: (landed(step), carry)[1], 0)

    squares = jnp.zeros((N, OC), f32)
    for p in range(E):
        x = r.got_e[p].reshape(N, OC).astype(f32)
        squares = squares + x * x
    inverse = lax.rsqrt(jnp.sum(squares, axis=1, keepdims=True) * (1.0 / D) + norm_eps)
    gate_sum = jnp.zeros((N, OC), f32)
    for p in range(E):
        at = slice(p * OC, (p + 1) * OC)
        x = r.got_e[p].reshape(N, OC).astype(f32)
        x = (x * inverse * r.ffn_gain[:, at]).astype(bf16)
        r.normed2[:, at] = x
        gate_sum = gate_sum + x.astype(f32) * r.branch_gate[:, at].astype(f32)
    branch = jax.nn.sigmoid(jnp.sum(gate_sum, axis=1, keepdims=True))

    own = r.normed2[:, pl.ds(pl.multiple_of(t * DQ, 128), DQ)]
    local["dense_gate"].wait()
    local["dense_up"].wait()
    whole_lanes = HQ % 128 == 0
    if not whole_lanes:
        for j in range(T):
            cols = slice(j * HQ, (j + 1) * HQ)
            r.all_f[j, 0] = dot(own, r.v_dense_gate[:, cols])
            r.all_f[j, 1] = dot(own, r.v_dense_up[:, cols])

    def dense_part(j, k):
        if not whole_lanes:
            return r.all_f[j, k]
        cols = pl.ds(pl.multiple_of(j * HQ, 128), HQ)
        return dot(own, (r.v_dense_gate, r.v_dense_up)[k][:, cols])

    f_core = [remote(r.st_f1.at[i], r.got_f1.at[i], one_of(i), None, (e, t1)) for i in range(2)]
    f_y = remote(r.st_f2, r.got_f2, one_of(2), None, (e, t2))
    for i, j in ((1, t3), (0, t1)):
        for k in range(2):
            r.st_f1[i, k] = dense_part(j, k).astype(bf16)
        f_core[i].start()
    for i, j in ((1, t2), (0, t)):
        for k in range(2):
            r.acc_f[i, k] = dense_part(j, k)

    rows = r.normed2[...]
    local["expert_gate"].wait()
    local["expert_up"].wait()
    local["expert_down"].wait()
    units = []
    for l in range(L):
        gate = jnp.minimum(dot(rows, r.v_expert_gate[l]), clamp_limit)
        up = jnp.clip(dot(rows, r.v_expert_up[l]), -clamp_limit, clamp_limit)
        units.append(((up + 1.0) * gate * jax.nn.sigmoid(swish_alpha * gate)).astype(bf16))
        if l == 0:
            f_core[1].wait_recv()
            r.st_f2[...] = (r.acc_f[1] + r.got_f1[1].astype(f32)).astype(bf16)
            f_y.start()

    def expert_part(j):
        out = None
        for l in range(L):
            scale = r.got_x[:, l].reshape(N, 128)[:, :1]
            cols = pl.ds(pl.multiple_of(j * DQ, 128), DQ)
            one = scale * dot(units[l], r.v_expert_down[l, :, cols])
            out = one if out is None else out + one
        return out

    m_core = [remote(r.st_m1.at[i], r.got_m1.at[i], one_of(3 + i), None, (e, t1)) for i in range(2)]
    m_y = remote(r.st_m2, r.got_m2, one_of(5), None, (e, t2))
    for i, j in ((1, t3), (0, t1)):
        r.st_m1[i] = expert_part(j).astype(bf16)
        m_core[i].start()
    for i, j in ((1, t2), (0, t)):
        r.acc_m[i] = expert_part(j)

    f_core[0].wait_recv()
    f_y.wait_recv()
    both = r.acc_f[0] + r.got_f1[0].astype(f32) + r.got_f2[...].astype(f32)
    hidden = (jax.nn.silu(both[0]) * both[1]).astype(bf16)
    r.got_h[t] = hidden
    h_y = remote(r.got_h.at[t], r.got_h.at[t], one_of(6), None, (e, t2))
    h_core = remote(r.got_h.at[t], r.got_h.at[t], one_of(7), None, (e, t1))
    h_cross = remote(r.got_h.at[t2], r.got_h.at[t2], one_of(8), None, (e, t1))
    h_y.start()
    h_core.start()
    m_core[1].wait_recv()
    m_core[0].wait_recv()
    r.st_m2[...] = (r.acc_m[1] + r.got_m1[1].astype(f32)).astype(bf16)
    m_y.start()
    h_y.wait_recv()
    h_cross.start()
    h_core.wait_recv()
    h_cross.wait_recv()
    local["dense_down"].wait()
    dense = dot(r.got_h[0], r.v_dense_down[0:HQ, :])
    for j in range(1, T):
        dense = dense + dot(r.got_h[j], r.v_dense_down[j * HQ : (j + 1) * HQ, :])
    m_y.wait_recv()
    final = branch * dense + r.acc_m[0] + r.got_m1[0].astype(f32) + r.got_m2[...].astype(f32)
    r.st_g[...] = final.astype(bf16).reshape(E, S, DQ)
    ep_loop(lambda step: ep_copy(r.st_g, r.got_g, sem_g, step).start())
    r.got_g[e] = r.st_g[e]

    def drain(step):
        ep_copy(r.st_a, r.got_a, sem_a, step).wait_send()
        answered(step).wait_send()
        ep_copy(r.st_r, r.got_r, sem_r, step).wait_send()
        ep_copy(r.st_k, r.got_k, sem_k, step).wait_send()
        ep_copy(r.st_x, r.got_x, sem_x, step).wait_send()
        c_copy(step).wait_send()
        e_copy(step).wait_send()

    ep_loop(drain)
    for step in range(1, T):
        d_copy(step).wait_send()

    def drain_all(step):
        src = source(step)
        pass_on(src, t, sem_ey, t2).wait_send()
        pass_on(src, t, sem_ec, t1).wait_send()
        pass_on(src, t2, sem_ez, t1).wait_send()

    lax.fori_loop(0, E, lambda step, carry: (drain_all(step), carry)[1], 0)
    for copy in (*f_core, f_y, *m_core, m_y, h_y, h_core, h_cross):
        copy.wait_send()

    ep_loop(lambda step: ep_copy(r.st_g, r.got_g, sem_g, step).wait())
    total = total_of(r.got_g)
    for k in range(GT):
        at = slice(k * OC, (k + 1) * OC)
        resid = r.got_e[t * GT + k, e].astype(f32)
        r.layer_out[:, at] = (resid + total[:, at]).astype(bf16)


def body(*args):
    E, T = lax.axis_size("ep"), lax.axis_size("tp")
    given = dict(zip(INPUTS, args))
    S, D = given["tokens"].shape
    N = E * S
    FE, QC = given["query_weight"].shape
    KC = given["key_weight"].shape[1]
    CL, HD = given["cache_keys"].shape[2:]
    G = QC // HD
    OC = given["out_weight"].shape[1]
    GT, DQ = E // T, D // T
    HQ = given["dense_gate"].shape[1] // T
    L = given["expert_gate"].shape[0]
    for name in ("attn_gain", "ffn_gain", "branch_gate"):
        given[name] = given[name].reshape(1, D)

    scratch = {}
    for name in STREAMED:
        scratch["v_" + name] = pltpu.VMEM(given[name].shape, given[name].dtype)

    def pair(name, shape, dtype=bf16):
        scratch["st_" + name] = pltpu.VMEM(shape, dtype)
        scratch["got_" + name] = pltpu.VMEM(shape, dtype)

    pair("a", (E, S, FE))
    pair("r", (E, S, FE))
    pair("q", (E, S, QC))
    pair("k", (E, S, 2 * KC))
    pair("x", (E, L, S, 128), f32)
    scratch["st_c"] = pltpu.VMEM((S, QC), bf16)
    scratch["got_c"] = pltpu.VMEM((E, S, QC), bf16)
    pair("d", (T, GT, S, OC))
    scratch["st_e"] = pltpu.VMEM((GT, S, OC), bf16)
    scratch["got_e"] = pltpu.VMEM((E, E, S, OC), bf16)
    pair("f1", (2, 2, N, HQ))
    pair("f2", (2, N, HQ))
    pair("m1", (2, N, DQ))
    pair("m2", (N, DQ))
    scratch["got_h"] = pltpu.VMEM((T, N, HQ), bf16)
    pair("g", (E, S, DQ))
    scratch["q_rows"] = pltpu.VMEM((S * G, HD), f32)
    scratch["mixed_rows"] = pltpu.VMEM((S * G, HD), f32)
    scratch["scores"] = pltpu.VMEM((S * G, CL), f32)
    scratch["normed2"] = pltpu.VMEM((N, D), bf16)
    scratch["acc_f"] = pltpu.VMEM((2, 2, N, HQ), f32)
    scratch["acc_m"] = pltpu.VMEM((2, N, DQ), f32)
    if HQ % 128:
        scratch["all_f"] = pltpu.VMEM((T, 2, N, HQ), f32)

    def sems(name, count):
        scratch[name + "_send"] = pltpu.SemaphoreType.DMA((count,))
        scratch[name + "_recv"] = pltpu.SemaphoreType.DMA((count,))

    for name in ("a", "q", "k", "r", "x", "c", "e", "g"):
        sems(name, E - 1)
    sems("d", T - 1)
    for name in ("ey", "ec", "ez"):
        sems(name, E)
    sems("one", 9)
    scratch["load_sem"] = pltpu.SemaphoreType.DMA((len(STREAMED),))

    in_specs = []
    for name in INPUTS:
        space = pltpu.VMEM
        if name in STREAMED:
            space = pltpu.HBM
        if name in SCALARS:
            space = pltpu.SMEM
        in_specs.append(pl.BlockSpec(memory_space=space))
    outs = ("layer_out", "new_keys", "new_values")
    names = INPUTS + outs + tuple(scratch)
    return pl.pallas_call(
        functools.partial(layer_kernel, names),
        out_shape=(
            jax.ShapeDtypeStruct((S, DQ), bf16),
            jax.ShapeDtypeStruct((S, KC), bf16),
            jax.ShapeDtypeStruct((S, KC), bf16),
        ),
        in_specs=in_specs,
        out_specs=(pl.BlockSpec(memory_space=pltpu.VMEM),) * 3,
        scratch_shapes=list(scratch.values()),
        compiler_params=pltpu.CompilerParams(
            collective_id=0, has_side_effects=True, vmem_limit_bytes=66_000_000
        ),
        name="layer",
    )(*(given[name] for name in INPUTS))


def solution(mesh):
    in_specs = (
        P("ep", None),
        P(),
        P("ep", "tp"),
        P("ep", "tp"),
        P("ep", "tp"),
        P("tp"),
        P("ep", "tp", None, None),
        P("ep", "tp", None, None),
        P("ep"),
        P("tp", "ep"),
        P(),
        P(),
        P("tp", "ep"),
        P("tp", "ep"),
        P("ep", "tp"),
        P("ep", None),
        P("ep", None),
        P("ep", None, "tp"),
        P("ep", None, "tp"),
        P("ep", "tp", None),
    )
    out_specs = (P("ep", "tp"), P("ep", "tp"), P("ep", "tp"))
    return jax.shard_map(body, mesh=mesh, in_specs=in_specs, out_specs=out_specs, check_vma=False)
```

```python
import functools
import jax
import jax.numpy as jnp
from jax import lax
from jax.experimental import pallas as pl
from jax.experimental.pallas import tpu as pltpu
from jax.sharding import PartitionSpec as P

norm_eps = 1e-05
clamp_limit = 7.0
swish_alpha = 1.702
f32, bf16 = jnp.float32, jnp.bfloat16
MESH = pl.DeviceIdType.MESH

INPUTS = (
    "tokens", "attn_gain", "query_weight", "key_weight", "value_weight", "break_bias",
    "cache_keys", "cache_values", "lengths", "out_weight", "ffn_gain", "branch_gate",
    "dense_gate", "dense_up", "dense_down", "route_ids", "route_weights", "expert_gate",
    "expert_up", "expert_down",
)
STREAMED = (
    "tokens", "attn_gain", "query_weight", "key_weight", "value_weight", "cache_keys", "cache_values", "out_weight",
    "dense_gate", "dense_up", "expert_gate", "expert_up", "expert_down", "dense_down",
)
FIRST = ("tokens", "attn_gain", "query_weight")
SCALARS = ("break_bias", "lengths")


def dot(a, b):
    return jnp.dot(a, b, preferred_element_type=f32)


class Refs:
    pass


def layer_kernel(names, *refs):
    r = Refs()
    for name, ref in zip(names, refs):
        setattr(r, name, ref)
    E, T = lax.axis_size("ep"), lax.axis_size("tp")
    e, t = lax.axis_index("ep"), lax.axis_index("tp")
    S, D = r.tokens.shape
    N = E * S
    bits = [1 << i for i in range((E - 1).bit_length())]
    FE = r.query_weight.shape[0]
    QC = r.query_weight.shape[1]
    KC = r.key_weight.shape[1]
    CL, HD = r.cache_keys.shape[2], r.cache_keys.shape[3]
    G = QC // HD
    OC = r.out_weight.shape[1]
    GT = E // T
    DQ = D // T
    HQ = r.dense_gate.shape[1] // T
    L = r.expert_gate.shape[0]
    t1 = t + 1 - 2 * lax.rem(t, 2)
    t2 = lax.rem(t + 2, T)
    t3 = lax.rem(t1 + 2, T)

    local = {
        name: pltpu.make_async_copy(getattr(r, name), getattr(r, "v_" + name), r.load_sem.at[i])
        for i, name in enumerate(STREAMED)
    }
    for name in FIRST:
        local[name].start()

    def peer_of(k):
        out = 0
        for bit in bits:
            out = out + bit * lax.rem(lax.rem(e // bit, 2) + (k // bit) % 2, 2)
        return out

    def ep_loop(fn):
        if E <= 8:
            for k in range(E - 1, 0, -1):
                fn(k)
        else:
            lax.fori_loop(1, E, lambda i, carry: (fn(E - i), carry)[1], 0)

    def all_loop(fn):
        fn(0)
        ep_loop(fn)

    barrier = pltpu.get_barrier_semaphore()

    def greet(where):
        pl.semaphore_signal(barrier, inc=1, device_id=where, device_id_type=MESH)

    ep_loop(lambda k: greet((peer_of(k), t)))
    for step in range(1, T):
        greet((e, lax.rem(t + step, T)))

    def remote(src, dst, sems, at, where):
        send, recv = sems
        return pltpu.make_async_remote_copy(
            src_ref=src,
            dst_ref=dst,
            send_sem=send if at is None else send.at[at],
            recv_sem=recv if at is None else recv.at[at],
            device_id=where,
            device_id_type=MESH,
        )

    def ep_copy(src, dst, sems, k, per_peer=True):
        peer = peer_of(k)
        return remote(src.at[peer] if per_peer else src, dst.at[e], sems, k - 1, (peer, t))

    sem_a = (r.a_send, r.a_recv)
    sem_q = (r.q_send, r.q_recv)
    sem_k = (r.k_send, r.k_recv)
    sem_r = (r.r_send, r.r_recv)
    sem_x = (r.x_send, r.x_recv)
    sem_c = (r.c_send, r.c_recv)
    sem_d = (r.d_send, r.d_recv)
    sem_e = (r.e_send, r.e_recv)
    sem_ey = (r.ey_send, r.ey_recv)
    sem_ec = (r.ec_send, r.ec_recv)
    sem_ez = (r.ez_send, r.ez_recv)
    sem_g = (r.g_send, r.g_recv)

    def one_of(at):
        return (r.one_send.at[at], r.one_recv.at[at])

    local["tokens"].wait()
    local["attn_gain"].wait()
    tokens = r.v_tokens[...].astype(f32)
    mean = jnp.mean(tokens * tokens, axis=-1, keepdims=True)
    normed = (tokens * lax.rsqrt(mean + norm_eps) * r.v_attn_gain[...]).astype(bf16)
    for p in range(E):
        r.st_a[p] = normed[:, p * FE : (p + 1) * FE]
    pl.semaphore_wait(barrier, E - 1 + T - 1)

    ep_loop(lambda step: ep_copy(r.st_a, r.got_a, sem_a, step).start())
    for name in STREAMED:
        if name not in FIRST:
            local[name].start()
    r.got_a[e] = r.st_a[e]
    for p in range(E):
        r.st_r[p] = r.v_tokens[:, p * FE : (p + 1) * FE]
    r.got_r[e] = r.st_r[e]
    local["query_weight"].wait()
    r.got_q[e] = dot(r.st_a[e], r.v_query_weight[...]).astype(bf16)

    def answered(k):
        src = peer_of(k)
        return remote(r.st_q.at[src], r.got_q.at[e], sem_q, k - 1, (src, t))

    def answer(k):
        ep_copy(r.st_a, r.got_a, sem_a, k).wait_recv()
        src = peer_of(k)
        r.st_q[src] = dot(r.got_a[src], r.v_query_weight[...]).astype(bf16)
        answered(k).start()

    ep_loop(answer)
    ep_loop(lambda k: ep_copy(r.st_r, r.got_r, sem_r, k).start())

    local["key_weight"].wait()
    local["value_weight"].wait()
    rows = r.got_a[...].reshape(N, FE)
    r.st_k[:, :, :KC] = dot(rows, r.v_key_weight[...]).astype(bf16).reshape(E, S, KC)
    r.st_k[:, :, KC:] = dot(rows, r.v_value_weight[...]).astype(bf16).reshape(E, S, KC)
    r.got_k[e] = r.st_k[e]
    diagonal = lax.broadcasted_iota(jnp.int32, (S, S), 0)
    diagonal = diagonal == lax.broadcasted_iota(jnp.int32, (S, S), 1)

    def column(line):
        spread = jnp.broadcast_to(line, (S, S))
        return jnp.sum(jnp.where(diagonal, spread, 0.0), axis=1, keepdims=True)

    picks = r.route_ids.shape[0]
    ids = [column(r.route_ids[k : k + 1, :].astype(f32)) for k in range(picks)]
    route = [column(r.route_weights[k : k + 1, :]) for k in range(picks)]

    def side(p, carry):
        for l in range(L):
            expert = jnp.full((S, 1), p * L + l, jnp.int32).astype(f32)
            own = jnp.zeros((S, 1), f32)
            for k in range(picks):
                own = own + jnp.where(ids[k] == expert, route[k], 0.0)
            r.st_x[p, l] = jnp.broadcast_to(own, (S, 128))
        return carry

    lax.fori_loop(0, E, side, 0)
    r.got_x[e] = r.st_x[e]
    for p in range(D // 128):
        r.gate_row[:, p * 128 : (p + 1) * 128] = r.branch_gate[p : p + 1, :].astype(f32)

    ep_loop(lambda k: answered(k).wait_recv())
    def total_of(got):
        def add(j, total):
            return total + got[j].astype(f32)

        return lax.fori_loop(1, E, add, got[0].astype(f32))

    queries = total_of(r.got_q).astype(bf16).astype(f32)
    for h in range(G):
        r.q_rows[pl.ds(h, S, stride=G), :] = queries[:, h * HD : (h + 1) * HD]

    tile = 8
    per = tile // G
    low = lax.broadcasted_iota(jnp.int32, (tile, 1), 0)

    def pick(parts):
        out = parts[0]
        for i in range(1, per):
            out = jnp.where(low >= i * G, parts[i], out)
        return out

    local["cache_keys"].wait()
    for i in range(S // per):
        q8 = r.q_rows[i * tile : (i + 1) * tile, :].astype(bf16)
        parts = [
            lax.dot_general(
                q8, r.v_cache_keys[i * per + j, 0], (((1,), (1,)), ((), ())),
                preferred_element_type=f32,
            )
            for j in range(per)
        ]
        r.scores[i * tile : (i + 1) * tile, :] = pick(parts)
    heads = S * G
    row = lax.broadcasted_iota(jnp.int32, (heads, 1), 0)
    length = jnp.zeros((heads, 1), jnp.int32)
    bias = jnp.zeros((heads, 1), f32)
    for s in range(S):
        length = jnp.where(row // G == s, r.lengths[s], length)
    for h in range(G):
        bias = jnp.where(lax.rem(row, G) == h, r.break_bias[h], bias)
    W = min(256, CL)
    later = lax.broadcasted_iota(jnp.int32, (W, W), 0)
    later = later > lax.broadcasted_iota(jnp.int32, (W, W), 1)
    later = jnp.where(later, 1.0, 0.0).astype(bf16)
    after = jnp.zeros((heads, 1), f32)
    for c in reversed(range(CL // W)):
        z = r.scores[:, c * W : (c + 1) * W] * HD ** (-0.5) + bias
        inside = lax.broadcasted_iota(jnp.int32, (heads, W), 1) + c * W < length
        soft = jnp.log1p(jnp.exp(-jnp.abs(z)))
        keep = jnp.where(inside, -(jnp.maximum(z, 0.0) + soft), 0.0)
        high = keep.astype(bf16)
        rest = keep - high.astype(f32)
        middle = rest.astype(bf16)
        least = (rest - middle.astype(f32)).astype(bf16)
        between = dot(high, later) + dot(middle, later) + dot(least, later) + after
        after = after + jnp.sum(keep, axis=1, keepdims=True)
        chance = jnp.exp(jnp.minimum(z, 0.0) - soft + between)
        r.scores[:, c * W : (c + 1) * W] = jnp.where(inside, chance, 0.0)
    local["cache_values"].wait()
    for i in range(S // per):
        w8 = r.scores[i * tile : (i + 1) * tile, :].astype(bf16)
        parts = [dot(w8, r.v_cache_values[i * per + j, 0]) for j in range(per)]
        r.mixed_rows[i * tile : (i + 1) * tile, :] = pick(parts)
    for h in range(G):
        r.st_c[:, h * HD : (h + 1) * HD] = r.mixed_rows[pl.ds(h, S, stride=G), :].astype(bf16)

    def c_copy(step):
        return ep_copy(r.st_c, r.got_c, sem_c, step, per_peer=False)

    ep_loop(lambda k: c_copy(k).start())
    ep_loop(lambda k: ep_copy(r.st_k, r.got_k, sem_k, k).start())
    ep_loop(lambda k: ep_copy(r.st_x, r.got_x, sem_x, k).start())
    r.got_c[e] = r.st_c[...]
    ep_loop(lambda k: ep_copy(r.st_r, r.got_r, sem_r, k).wait_recv())
    ep_loop(lambda k: answered(k).wait_send())
    if DQ == QC:
        r.st_g = r.st_q
    local["out_weight"].wait()
    ep_loop(lambda step: c_copy(step).wait_recv())
    part = dot(r.got_c[...].reshape(N, QC), r.v_out_weight[...]).astype(bf16)
    r.st_d[...] = part.reshape(T, GT, S, OC)

    def d_copy(step):
        peer = lax.rem(t + step, T)
        return remote(r.st_d.at[peer], r.got_d.at[t], sem_d, step - 1, (e, peer))

    for step in range(1, T):
        d_copy(step).start()
    r.got_d[t] = r.st_d[t]
    for step in range(1, T):
        d_copy(step).wait_recv()
    mixed = r.got_d[0].astype(f32)
    for j in range(1, T):
        mixed = mixed + r.got_d[j].astype(f32)
    mixed = mixed.astype(bf16).astype(f32)

    mine = pl.ds(t * GT, GT)
    r.st_e[...] = (r.got_r[mine].astype(f32) + mixed).astype(bf16)

    def e_copy(k):
        return remote(r.st_e, r.got_e.at[e, mine], sem_e, k - 1, (peer_of(k), t))

    ep_loop(lambda step: e_copy(step).start())
    r.got_e[e, mine] = r.st_e[...]

    def pass_on(src, group, sems, peer):
        block = r.got_e.at[src, pl.ds(group * GT, GT)]
        return remote(block, block, sems, src, (e, peer))

    remote(r.st_e, r.got_e.at[e, mine], sem_ey, e, (e, t2)).start()
    remote(r.st_e, r.got_e.at[e, mine], sem_ec, e, (e, t1)).start()

    def forward(step):
        e_copy(step).wait_recv()
        src = peer_of(step)
        pass_on(src, t, sem_ey, t2).start()
        pass_on(src, t, sem_ec, t1).start()

    ep_loop(forward)

    def cross(step):
        src = peer_of(step)
        pass_on(src, t, sem_ey, t2).wait_recv()
        pass_on(src, t2, sem_ez, t1).start()

    all_loop(cross)

    def landed(step):
        src = peer_of(step)
        pass_on(src, t, sem_ec, t1).wait_recv()
        pass_on(src, t2, sem_ez, t1).wait_recv()

    all_loop(landed)

    squares = jnp.zeros((N, OC), f32)
    for p in range(E):
        x = r.got_e[p].reshape(N, OC).astype(f32)
        squares = squares + x * x
    inverse = lax.rsqrt(jnp.sum(squares, axis=1, keepdims=True) * (1.0 / D) + norm_eps)
    gate_sum = jnp.zeros((N, OC), f32)
    for p in range(E):
        at = slice(p * OC, (p + 1) * OC)
        x = r.got_e[p].reshape(N, OC).astype(f32)
        x = (x * inverse * r.ffn_gain[:, at]).astype(bf16)
        r.normed2[:, at] = x
        gate_sum = gate_sum + x.astype(f32) * r.gate_row[:, at]
    branch = jax.nn.sigmoid(jnp.sum(gate_sum, axis=1, keepdims=True))

    own = r.normed2[:, pl.ds(pl.multiple_of(t * DQ, 128), DQ)]
    local["dense_gate"].wait()
    local["dense_up"].wait()
    whole_lanes = HQ % 128 == 0
    if not whole_lanes:
        for j in range(T):
            cols = slice(j * HQ, (j + 1) * HQ)
            r.all_f[j, 0] = dot(own, r.v_dense_gate[:, cols])
            r.all_f[j, 1] = dot(own, r.v_dense_up[:, cols])

    def dense_part(j, k):
        if not whole_lanes:
            return r.all_f[j, k]
        cols = pl.ds(pl.multiple_of(j * HQ, 128), HQ)
        return dot(own, (r.v_dense_gate, r.v_dense_up)[k][:, cols])

    f_core = [remote(r.st_f1.at[i], r.got_f1.at[i], one_of(i), None, (e, t1)) for i in range(2)]
    f_y = remote(r.st_f2, r.got_f2, one_of(2), None, (e, t2))
    for i, j in ((1, t3), (0, t1)):
        for k in range(2):
            r.st_f1[i, k] = dense_part(j, k).astype(bf16)
        f_core[i].start()
    for i, j in ((1, t2), (0, t)):
        for k in range(2):
            r.acc_f[i, k] = dense_part(j, k)

    rows = r.normed2[...]
    local["expert_gate"].wait()
    local["expert_up"].wait()
    local["expert_down"].wait()
    units = []
    for l in range(L):
        gate = jnp.minimum(dot(rows, r.v_expert_gate[l]), clamp_limit)
        up = jnp.clip(dot(rows, r.v_expert_up[l]), -clamp_limit, clamp_limit)
        units.append(((up + 1.0) * gate * jax.nn.sigmoid(swish_alpha * gate)).astype(bf16))
        if l == 0:
            f_core[1].wait_recv()
            r.st_f2[...] = (r.acc_f[1] + r.got_f1[1].astype(f32)).astype(bf16)
            f_y.start()

    ep_loop(lambda k: ep_copy(r.st_x, r.got_x, sem_x, k).wait_recv())

    def expert_part(j):
        out = None
        for l in range(L):
            scale = r.got_x[:, l].reshape(N, 128)[:, :1]
            cols = pl.ds(pl.multiple_of(j * DQ, 128), DQ)
            one = scale * dot(units[l], r.v_expert_down[l, :, cols])
            out = one if out is None else out + one
        return out

    m_core = [remote(r.st_m1.at[i], r.got_m1.at[i], one_of(3 + i), None, (e, t1)) for i in range(2)]
    half = DQ // 2
    m_y = [remote(r.st_m2.at[i], r.got_m2.at[i], one_of(9 + i), None, (e, t2)) for i in range(2)]

    def m_send(i):
        cols = slice(i * half, (i + 1) * half)
        r.st_m2[i] = (r.acc_m[1, :, cols] + r.got_m1[1, :, cols].astype(f32)).astype(bf16)
        m_y[i].start()

    for i, j in ((1, t3), (0, t1)):
        r.st_m1[i] = expert_part(j).astype(bf16)
        m_core[i].start()
    r.acc_m[1] = expert_part(t2)
    m_core[1].wait_recv()
    m_send(0)
    r.acc_m[0] = expert_part(t)

    ep_loop(lambda k: ep_copy(r.st_k, r.got_k, sem_k, k).wait_recv())
    new_rows = total_of(r.got_k).astype(bf16)
    r.outs[:, DQ:] = new_rows
    f_core[0].wait_recv()
    f_y.wait_recv()
    both = r.acc_f[0] + r.got_f1[0].astype(f32) + r.got_f2[...].astype(f32)
    hidden = (jax.nn.silu(both[0]) * both[1]).astype(bf16)
    r.got_h[t] = hidden
    h_y = remote(r.got_h.at[t], r.got_h.at[t], one_of(6), None, (e, t2))
    h_core = remote(r.got_h.at[t], r.got_h.at[t], one_of(7), None, (e, t1))
    h_cross = remote(r.got_h.at[t2], r.got_h.at[t2], one_of(8), None, (e, t1))
    h_y.start()
    h_core.start()
    m_send(1)
    ep_loop(lambda k: ep_copy(r.st_x, r.got_x, sem_x, k).wait_send())
    h_y.wait_recv()
    h_cross.start()
    h_core.wait_recv()
    h_cross.wait_recv()
    local["dense_down"].wait()
    dense = dot(r.got_h[0], r.v_dense_down[0:HQ, :])
    for j in range(1, T):
        dense = dense + dot(r.got_h[j], r.v_dense_down[j * HQ : (j + 1) * HQ, :])
    m_core[0].wait_recv()
    for i in range(2):
        cols = slice(i * half, (i + 1) * half)
        m_y[i].wait_recv()
        final = branch * dense[:, cols] + r.acc_m[0, :, cols] + r.got_m1[0, :, cols].astype(f32)
        final = final + r.got_m2[i].astype(f32)
        r.st_g[:, :, cols] = final.astype(bf16).reshape(E, S, half)
    ep_loop(lambda step: ep_copy(r.st_g, r.got_g, sem_g, step).start())
    r.got_g[e] = r.st_g[e]

    def drain(step):
        ep_copy(r.st_a, r.got_a, sem_a, step).wait_send()
        ep_copy(r.st_r, r.got_r, sem_r, step).wait_send()
        ep_copy(r.st_k, r.got_k, sem_k, step).wait_send()
        c_copy(step).wait_send()
        e_copy(step).wait_send()

    ep_loop(drain)
    for step in range(1, T):
        d_copy(step).wait_send()

    def drain_all(step):
        src = peer_of(step)
        pass_on(src, t, sem_ey, t2).wait_send()
        pass_on(src, t, sem_ec, t1).wait_send()
        pass_on(src, t2, sem_ez, t1).wait_send()

    all_loop(drain_all)
    for copy in (*f_core, f_y, *m_core, *m_y, h_y, h_core, h_cross):
        copy.wait_send()

    ep_loop(lambda step: ep_copy(r.st_g, r.got_g, sem_g, step).wait())
    total = total_of(r.got_g)
    for k in range(GT):
        at = slice(k * OC, (k + 1) * OC)
        resid = r.got_e[t * GT + k, e].astype(f32)
        r.outs[:, at] = (resid + total[:, at]).astype(bf16)


def vmem_grant(scratch):
    total = 6 << 20
    for ref in scratch.values():
        if len(ref.shape) > 1:
            rows = 1
            for size in ref.shape[:-1]:
                rows *= size
            total += rows * -(-ref.shape[-1] // 128) * 128 * jnp.dtype(ref.dtype).itemsize
    return min(total, 67_043_328)


def body(*args):
    E, T = lax.axis_size("ep"), lax.axis_size("tp")
    given = dict(zip(INPUTS, args))
    S, D = given["tokens"].shape
    N = E * S
    FE, QC = given["query_weight"].shape
    KC = given["key_weight"].shape[1]
    CL, HD = given["cache_keys"].shape[2:]
    G = QC // HD
    OC = given["out_weight"].shape[1]
    GT, DQ = E // T, D // T
    HQ = given["dense_gate"].shape[1] // T
    L = given["expert_gate"].shape[0]
    for name in ("attn_gain", "ffn_gain"):
        given[name] = given[name].reshape(1, D)
    given["branch_gate"] = given["branch_gate"].reshape(D // 128, 128)
    for name in ("route_ids", "route_weights"):
        given[name] = given[name].T

    scratch = {}
    for name in STREAMED:
        scratch["v_" + name] = pltpu.VMEM(given[name].shape, given[name].dtype)

    def pair(name, shape, dtype=bf16):
        scratch["st_" + name] = pltpu.VMEM(shape, dtype)
        scratch["got_" + name] = pltpu.VMEM(shape, dtype)

    pair("a", (E, S, FE))
    pair("r", (E, S, FE))
    pair("q", (E, S, QC))
    pair("k", (E, S, 2 * KC))
    pair("x", (E, L, S, 128), f32)
    scratch["st_c"] = pltpu.VMEM((S, QC), bf16)
    scratch["got_c"] = pltpu.VMEM((E, S, QC), bf16)
    pair("d", (T, GT, S, OC))
    scratch["st_e"] = pltpu.VMEM((GT, S, OC), bf16)
    scratch["got_e"] = pltpu.VMEM((E, E, S, OC), bf16)
    pair("f1", (2, 2, N, HQ))
    pair("f2", (2, N, HQ))
    pair("m1", (2, N, DQ))
    pair("m2", (2, N, DQ // 2))
    scratch["gate_row"] = pltpu.VMEM((1, D), f32)
    scratch["got_h"] = pltpu.VMEM((T, N, HQ), bf16)
    scratch["got_g"] = pltpu.VMEM((E, S, DQ), bf16)
    if DQ != QC:
        scratch["st_g"] = pltpu.VMEM((E, S, DQ), bf16)
    scratch["q_rows"] = pltpu.VMEM((S * G, HD), f32)
    scratch["mixed_rows"] = pltpu.VMEM((S * G, HD), f32)
    scratch["scores"] = pltpu.VMEM((S * G, CL), f32)
    scratch["normed2"] = pltpu.VMEM((N, D), bf16)
    scratch["acc_f"] = pltpu.VMEM((2, 2, N, HQ), f32)
    scratch["acc_m"] = pltpu.VMEM((2, N, DQ), f32)
    if HQ % 128:
        scratch["all_f"] = pltpu.VMEM((T, 2, N, HQ), f32)

    def sems(name, count):
        scratch[name + "_send"] = pltpu.SemaphoreType.DMA((count,))
        scratch[name + "_recv"] = pltpu.SemaphoreType.DMA((count,))

    for name in ("a", "q", "k", "r", "x", "c", "e", "g"):
        sems(name, E - 1)
    sems("d", T - 1)
    for name in ("ey", "ec", "ez"):
        sems(name, E)
    sems("one", 11)
    scratch["load_sem"] = pltpu.SemaphoreType.DMA((len(STREAMED),))

    in_specs = []
    for name in INPUTS:
        space = pltpu.VMEM
        if name in STREAMED:
            space = pltpu.HBM
        if name in SCALARS:
            space = pltpu.SMEM
        in_specs.append(pl.BlockSpec(memory_space=space))
    names = INPUTS + ("outs",) + tuple(scratch)
    packed = pl.pallas_call(
        functools.partial(layer_kernel, names),
        out_shape=jax.ShapeDtypeStruct((S, DQ + 2 * KC), bf16),
        in_specs=in_specs,
        out_specs=pl.BlockSpec(memory_space=pltpu.VMEM),
        scratch_shapes=list(scratch.values()),
        compiler_params=pltpu.CompilerParams(
            collective_id=0, has_side_effects=True, vmem_limit_bytes=vmem_grant(scratch)
        ),
        name="layer",
    )(*(given[name] for name in INPUTS))

    def part(packed_ref, layer_ref, keys_ref, values_ref):
        layer_ref[...] = packed_ref[:, :DQ]
        keys_ref[...] = packed_ref[:, DQ : DQ + KC]
        values_ref[...] = packed_ref[:, DQ + KC :]

    return pl.pallas_call(
        part,
        out_shape=tuple(jax.ShapeDtypeStruct((S, width), bf16) for width in (DQ, KC, KC)),
        in_specs=[pl.BlockSpec(memory_space=pltpu.VMEM)],
        out_specs=(pl.BlockSpec(memory_space=pltpu.VMEM),) * 3,
        name="part",
    )(packed)


def solution(mesh):
    in_specs = (
        P("ep", None),
        P(),
        P("ep", "tp"),
        P("ep", "tp"),
        P("ep", "tp"),
        P("tp"),
        P("ep", "tp", None, None),
        P("ep", "tp", None, None),
        P("ep"),
        P("tp", "ep"),
        P(),
        P(),
        P("tp", "ep"),
        P("tp", "ep"),
        P("ep", "tp"),
        P("ep", None),
        P("ep", None),
        P("ep", None, "tp"),
        P("ep", None, "tp"),
        P("ep", "tp", None),
    )
    out_specs = (P("ep", "tp"), P("ep", "tp"), P("ep", "tp"))
    return jax.shard_map(body, mesh=mesh, in_specs=in_specs, out_specs=out_specs, check_vma=False)
```

```python
import functools
import jax
import jax.numpy as jnp
from jax import lax
from jax.experimental import pallas as pl
from jax.experimental.pallas import tpu as pltpu
from jax.sharding import PartitionSpec as P

norm_eps = 1e-05
clamp_limit = 7.0
swish_alpha = 1.702
f32, bf16 = jnp.float32, jnp.bfloat16
MESH = pl.DeviceIdType.MESH

INPUTS = (
    "tokens", "attn_gain", "query_weight", "key_weight", "value_weight", "break_bias",
    "cache_keys", "cache_values", "lengths", "out_weight", "ffn_gain", "branch_gate",
    "dense_gate", "dense_up", "dense_down", "route_ids", "route_weights", "expert_gate",
    "expert_up", "expert_down",
)
FIRST = ("tokens", "attn_gain", "query_weight", "out_weight")
SCALARS = ("break_bias", "lengths")
LATER = (
    "route_ids", "route_weights", "branch_gate", "ffn_gain", "key_weight", "value_weight",
    "cache_keys", "dense_gate", "dense_up", "cache_values", "expert_gate", "expert_up",
    "expert_down", "dense_down",
)
STREAMED = FIRST + SCALARS + LATER


def dot(a, b):
    return jnp.dot(a, b, preferred_element_type=f32)


class Refs:
    pass


def layer_kernel(names, *refs):
    r = Refs()
    for name, ref in zip(names, refs):
        setattr(r, name, ref)
    E, T = lax.axis_size("ep"), lax.axis_size("tp")
    e, t = lax.axis_index("ep"), lax.axis_index("tp")
    S, D = r.tokens.shape
    N = E * S
    bits = [1 << i for i in range((E - 1).bit_length())]
    FE = r.query_weight.shape[0]
    QC = r.query_weight.shape[1]
    KC = r.key_weight.shape[1]
    CL, HD = r.cache_keys.shape[2], r.cache_keys.shape[3]
    G = QC // HD
    OC = r.out_weight.shape[1]
    GT = E // T
    DQ = D // T
    HQ = r.dense_gate.shape[1] // T
    L = r.expert_gate.shape[0]
    t1 = t + 1 - 2 * lax.rem(t, 2)
    t2 = lax.rem(t + 2, T)
    t3 = lax.rem(t1 + 2, T)

    local = {}
    for i, name in enumerate(STREAMED):
        into = r.wo_all.at[t] if name == "out_weight" else getattr(r, "v_" + name)
        local[name] = pltpu.make_async_copy(getattr(r, name), into, r.load_sem.at[i])
    for name in FIRST:
        local[name].start()

    def peer_of(k):
        out = 0
        for bit in bits:
            out = out + bit * lax.rem(lax.rem(e // bit, 2) + (k // bit) % 2, 2)
        return out

    def ep_loop(fn):
        if E <= 8:
            for k in range(E - 1, 0, -1):
                fn(k)
        else:
            lax.fori_loop(1, E, lambda i, carry: (fn(E - i), carry)[1], 0)

    def all_loop(fn):
        fn(0)
        ep_loop(fn)

    barrier = pltpu.get_barrier_semaphore()

    def greet(where):
        pl.semaphore_signal(barrier, inc=1, device_id=where, device_id_type=MESH)

    ep_loop(lambda k: greet((peer_of(k), t)))
    for step in range(1, T):
        greet((e, lax.rem(t + step, T)))

    owner = e // GT
    here = owner == t

    def group_loop(fn):
        def one(i, carry):
            fn(lax.rem(i, T), i // T)
            return carry

        lax.fori_loop(0, E, one, 0)

    def greet_group(source_t, j):
        group = t * GT + j

        @pl.when(jnp.logical_or(group != e, source_t != t))
        def _():
            greet((group, source_t))

    group_loop(greet_group)

    def remote(src, dst, sems, at, where):
        send, recv = sems
        return pltpu.make_async_remote_copy(
            src_ref=src,
            dst_ref=dst,
            send_sem=send if at is None else send.at[at],
            recv_sem=recv if at is None else recv.at[at],
            device_id=where,
            device_id_type=MESH,
        )

    def ep_copy(src, dst, sems, k, per_peer=True):
        peer = peer_of(k)
        return remote(src.at[peer] if per_peer else src, dst.at[e], sems, k - 1, (peer, t))

    sem_a = (r.a_send, r.a_recv)
    sem_q = (r.q_send, r.q_recv)
    sem_k = (r.k_send, r.k_recv)
    sem_r = (r.r_send, r.r_recv)
    sem_x = (r.x_send, r.x_recv)
    sem_c = (r.c_send, r.c_recv)
    sem_e = (r.e_send, r.e_recv)
    sem_ey = (r.ey_send, r.ey_recv)
    sem_ec = (r.ec_send, r.ec_recv)
    sem_ez = (r.ez_send, r.ez_recv)
    sem_g = (r.g_send, r.g_recv)

    def one_of(at):
        return (r.one_send.at[at], r.one_recv.at[at])

    local["tokens"].wait()
    local["attn_gain"].wait()
    tokens = r.v_tokens[...].astype(f32)
    mean = jnp.mean(tokens * tokens, axis=-1, keepdims=True)
    normed = (tokens * lax.rsqrt(mean + norm_eps) * r.v_attn_gain[...]).astype(bf16)
    for p in range(E):
        r.st_a[p] = normed[:, p * FE : (p + 1) * FE]
    pl.semaphore_wait(barrier, E - 1 + T - 1 + E - jnp.where(here, 1, 0))

    ep_loop(lambda step: ep_copy(r.st_a, r.got_a, sem_a, step).start())
    for name in SCALARS + LATER:
        local[name].start()
    r.got_a[e] = r.st_a[e]
    for p in range(E):
        r.st_r[p] = r.v_tokens[:, p * FE : (p + 1) * FE]
    r.got_r[e] = r.st_r[e]
    def wo_copy(block, at, peer):
        block = r.wo_all.at[block]
        return remote(block, block, one_of(at), None, (e, peer))

    wo_y, wo_core, wo_cross = wo_copy(t, 0, t2), wo_copy(t, 1, t1), wo_copy(t2, 3, t1)
    local["out_weight"].wait()
    wo_y.start()
    wo_core.start()
    local["query_weight"].wait()
    r.got_q[e] = dot(r.st_a[e], r.v_query_weight[...]).astype(bf16)

    def answered(k):
        src = peer_of(k)
        return remote(r.st_q.at[src], r.got_q.at[e], sem_q, k - 1, (src, t))

    def answer(k):
        ep_copy(r.st_a, r.got_a, sem_a, k).wait_recv()
        src = peer_of(k)
        r.st_q[src] = dot(r.got_a[src], r.v_query_weight[...]).astype(bf16)
        answered(k).start()

    ep_loop(answer)
    local["key_weight"].wait()
    local["value_weight"].wait()
    rows = r.got_a[...].reshape(N, FE)
    r.st_k[:, :, :KC] = dot(rows, r.v_key_weight[...]).astype(bf16).reshape(E, S, KC)
    r.st_k[:, :, KC:] = dot(rows, r.v_value_weight[...]).astype(bf16).reshape(E, S, KC)
    r.got_k[e] = r.st_k[e]
    diagonal = lax.broadcasted_iota(jnp.int32, (S, S), 0)
    diagonal = diagonal == lax.broadcasted_iota(jnp.int32, (S, S), 1)

    def column(line):
        spread = jnp.broadcast_to(line, (S, S))
        return jnp.sum(jnp.where(diagonal, spread, 0.0), axis=1, keepdims=True)

    for name in ("route_ids", "route_weights", "branch_gate", "ffn_gain"):
        local[name].wait()
    picks = r.route_ids.shape[0]
    ids = [column(r.v_route_ids[k : k + 1, :].astype(f32)) for k in range(picks)]
    route = [column(r.v_route_weights[k : k + 1, :]) for k in range(picks)]

    def side(p, carry):
        for l in range(L):
            expert = jnp.full((S, 1), p * L + l, jnp.int32).astype(f32)
            own = jnp.zeros((S, 1), f32)
            for k in range(picks):
                own = own + jnp.where(ids[k] == expert, route[k], 0.0)
            r.st_x[p, l] = jnp.broadcast_to(own, (S, 128))
        return carry

    lax.fori_loop(0, E, side, 0)
    r.got_x[e] = r.st_x[e]
    for p in range(D // 128):
        r.gate_row[:, p * 128 : (p + 1) * 128] = r.v_branch_gate[p : p + 1, :].astype(f32)

    dense_swap = [
        remote(r.v_dense_gate, r.o_dense_gate, one_of(4), None, (e, t1)),
        remote(r.v_dense_up, r.o_dense_up, one_of(5), None, (e, t1)),
    ]
    for name in ("dense_gate", "dense_up"):
        local[name].wait()
    for copy in dense_swap:
        copy.start()

    ep_loop(lambda k: answered(k).wait_recv())
    ep_loop(lambda k: ep_copy(r.st_r, r.got_r, sem_r, k).start())
    ep_loop(lambda k: ep_copy(r.st_x, r.got_x, sem_x, k).start())
    wo_y.wait_recv()
    wo_cross.start()
    def total_of(got):
        def add(j, total):
            return total + got[j].astype(f32)

        return lax.fori_loop(1, E, add, got[0].astype(f32))

    queries = total_of(r.got_q).astype(bf16).astype(f32)
    for h in range(G):
        r.q_rows[pl.ds(h, S, stride=G), :] = queries[:, h * HD : (h + 1) * HD]

    tile = 8
    per = tile // G
    low = lax.broadcasted_iota(jnp.int32, (tile, 1), 0)

    def pick(parts):
        out = parts[0]
        for i in range(1, per):
            out = jnp.where(low >= i * G, parts[i], out)
        return out

    local["cache_keys"].wait()
    for i in range(S // per):
        q8 = r.q_rows[i * tile : (i + 1) * tile, :].astype(bf16)
        parts = [
            lax.dot_general(
                q8, r.v_cache_keys[i * per + j, 0], (((1,), (1,)), ((), ())),
                preferred_element_type=f32,
            )
            for j in range(per)
        ]
        r.scores[i * tile : (i + 1) * tile, :] = pick(parts)
    for name in SCALARS:
        local[name].wait()
    heads = S * G
    row = lax.broadcasted_iota(jnp.int32, (heads, 1), 0)
    length = jnp.zeros((heads, 1), jnp.int32)
    bias = jnp.zeros((heads, 1), f32)
    for s in range(S):
        length = jnp.where(row // G == s, r.v_lengths[s], length)
    for h in range(G):
        bias = jnp.where(lax.rem(row, G) == h, r.v_break_bias[h], bias)
    W = min(256, CL)
    later = lax.broadcasted_iota(jnp.int32, (W, W), 0)
    later = later > lax.broadcasted_iota(jnp.int32, (W, W), 1)
    later = jnp.where(later, 1.0, 0.0).astype(bf16)
    after = jnp.zeros((heads, 1), f32)
    for c in reversed(range(CL // W)):
        z = r.scores[:, c * W : (c + 1) * W] * HD ** (-0.5) + bias
        inside = lax.broadcasted_iota(jnp.int32, (heads, W), 1) + c * W < length
        soft = jnp.log1p(jnp.exp(-jnp.abs(z)))
        keep = jnp.where(inside, -(jnp.maximum(z, 0.0) + soft), 0.0)
        high = keep.astype(bf16)
        rest = keep - high.astype(f32)
        middle = rest.astype(bf16)
        least = (rest - middle.astype(f32)).astype(bf16)
        between = dot(high, later) + dot(middle, later) + dot(least, later) + after
        after = after + jnp.sum(keep, axis=1, keepdims=True)
        chance = jnp.exp(jnp.minimum(z, 0.0) - soft + between)
        r.scores[:, c * W : (c + 1) * W] = jnp.where(inside, chance, 0.0)
    local["cache_values"].wait()
    for i in range(S // per):
        w8 = r.scores[i * tile : (i + 1) * tile, :].astype(bf16)
        parts = [dot(w8, r.v_cache_values[i * per + j, 0]) for j in range(per)]
        r.mixed_rows[i * tile : (i + 1) * tile, :] = pick(parts)
    for h in range(G):
        r.st_c[:, h * HD : (h + 1) * HD] = r.mixed_rows[pl.ds(h, S, stride=G), :].astype(bf16)

    def c_copy(k):
        peer = peer_of(k)
        block = r.got_c.at[t, lax.rem(e, GT)]
        return pltpu.make_async_remote_copy(
            src_ref=r.st_c,
            dst_ref=block,
            send_sem=r.c_send.at[k],
            recv_sem=r.c_recv.at[t * GT + lax.rem(e, GT)],
            device_id=(peer, owner),
            device_id_type=MESH,
        )

    def c_arrival(source_t, j):
        return pltpu.make_async_remote_copy(
            src_ref=r.st_c,
            dst_ref=r.got_c.at[source_t, j],
            send_sem=r.c_send.at[0],
            recv_sem=r.c_recv.at[source_t * GT + j],
            device_id=(t * GT + j, source_t),
            device_id_type=MESH,
        )

    ep_loop(lambda k: c_copy(k).start())

    @pl.when(jnp.logical_not(here))
    def _():
        c_copy(0).start()

    @pl.when(here)
    def _():
        r.got_c[t, lax.rem(e, GT)] = r.st_c[...]

    ep_loop(lambda k: ep_copy(r.st_r, r.got_r, sem_r, k).wait_recv())
    ep_loop(lambda k: answered(k).wait_send())
    if DQ == QC:
        r.st_g = r.st_q
    wo_core.wait_recv()
    wo_cross.wait_recv()

    def c_wait(source_t, j):
        @pl.when(jnp.logical_or(t * GT + j != e, source_t != t))
        def _():
            c_arrival(source_t, j).wait_recv()

    group_loop(c_wait)
    mixed = dot(r.got_c[0].reshape(GT * S, QC), r.wo_all[0])
    for j in range(1, T):
        mixed = mixed + dot(r.got_c[j].reshape(GT * S, QC), r.wo_all[j])
    mixed = mixed.astype(bf16).astype(f32).reshape(GT, S, OC)

    mine = pl.ds(t * GT, GT)
    r.st_e[...] = (r.got_r[mine].astype(f32) + mixed).astype(bf16)

    def e_copy(k):
        return remote(r.st_e, r.got_e.at[e, mine], sem_e, k - 1, (peer_of(k), t))

    ep_loop(lambda step: e_copy(step).start())
    r.got_e[e, mine] = r.st_e[...]

    def pass_on(src, group, sems, peer):
        block = r.got_e.at[src, pl.ds(group * GT, GT)]
        return remote(block, block, sems, src, (e, peer))

    remote(r.st_e, r.got_e.at[e, mine], sem_ey, e, (e, t2)).start()
    remote(r.st_e, r.got_e.at[e, mine], sem_ec, e, (e, t1)).start()

    def forward(step):
        e_copy(step).wait_recv()
        src = peer_of(step)
        pass_on(src, t, sem_ey, t2).start()
        pass_on(src, t, sem_ec, t1).start()

    ep_loop(forward)

    def cross(step):
        src = peer_of(step)
        pass_on(src, t, sem_ey, t2).wait_recv()
        pass_on(src, t2, sem_ez, t1).start()

    all_loop(cross)

    def landed(step):
        src = peer_of(step)
        pass_on(src, t, sem_ec, t1).wait_recv()
        pass_on(src, t2, sem_ez, t1).wait_recv()

    all_loop(landed)

    squares = jnp.zeros((N, OC), f32)
    for p in range(E):
        x = r.got_e[p].reshape(N, OC).astype(f32)
        squares = squares + x * x
    inverse = lax.rsqrt(jnp.sum(squares, axis=1, keepdims=True) * (1.0 / D) + norm_eps)
    gate_sum = jnp.zeros((N, OC), f32)
    for p in range(E):
        at = slice(p * OC, (p + 1) * OC)
        x = r.got_e[p].reshape(N, OC).astype(f32)
        x = (x * inverse * r.v_ffn_gain[:, at]).astype(bf16)
        r.normed2[:, at] = x
        gate_sum = gate_sum + x.astype(f32) * r.gate_row[:, at]
    branch = jax.nn.sigmoid(jnp.sum(gate_sum, axis=1, keepdims=True))

    own = r.normed2[:, pl.ds(pl.multiple_of(t * DQ, 128), DQ)]
    other = r.normed2[:, pl.ds(pl.multiple_of(t1 * DQ, 128), DQ)]
    for copy in dense_swap:
        copy.wait_recv()
    pairs = ((r.v_dense_gate, r.o_dense_gate), (r.v_dense_up, r.o_dense_up))
    whole_lanes = HQ % 128 == 0
    if not whole_lanes:
        for j in range(T):
            cols = slice(j * HQ, (j + 1) * HQ)
            for k in range(2):
                r.all_f[j, k] = dot(own, pairs[k][0][:, cols]) + dot(other, pairs[k][1][:, cols])

    def dense_part(j, k):
        if not whole_lanes:
            return r.all_f[j, k]
        cols = pl.ds(pl.multiple_of(j * HQ, 128), HQ)
        return dot(own, pairs[k][0][:, cols]) + dot(other, pairs[k][1][:, cols])

    f_y = [remote(r.st_f2.at[h], r.got_f2.at[h], one_of((2, 13)[h]), None, (e, t2)) for h in range(2)]
    for k in range(2):
        r.st_f2[:, k] = dense_part(t2, k).astype(bf16).reshape(2, N // 2, HQ)
    for copy in f_y:
        copy.start()
    ep_loop(lambda k: ep_copy(r.st_k, r.got_k, sem_k, k).start())
    for k in range(2):
        r.acc_f[k] = dense_part(t, k)

    rows = r.normed2[...]
    local["expert_gate"].wait()
    local["expert_up"].wait()
    local["expert_down"].wait()
    units = []
    for l in range(L):
        gate = jnp.minimum(dot(rows, r.v_expert_gate[l]), clamp_limit)
        up = jnp.clip(dot(rows, r.v_expert_up[l]), -clamp_limit, clamp_limit)
        units.append(((up + 1.0) * gate * jax.nn.sigmoid(swish_alpha * gate)).astype(bf16))

    ep_loop(lambda k: ep_copy(r.st_x, r.got_x, sem_x, k).wait_recv())

    def expert_part(j):
        out = None
        for l in range(L):
            scale = r.got_x[:, l].reshape(N, 128)[:, :1]
            cols = pl.ds(pl.multiple_of(j * DQ, 128), DQ)
            one = scale * dot(units[l], r.v_expert_down[l, :, cols])
            out = one if out is None else out + one
        return out

    m_core = [remote(r.st_m1.at[i], r.got_m1.at[i], one_of(11 + i), None, (e, t1)) for i in range(2)]
    half = DQ // 2
    m_y = [remote(r.st_m2.at[i], r.got_m2.at[i], one_of(9 + i), None, (e, t2)) for i in range(2)]

    def m_send(i):
        cols = slice(i * half, (i + 1) * half)
        r.st_m2[i] = (r.acc_m[1, :, cols] + r.got_m1[1, :, cols].astype(f32)).astype(bf16)
        m_y[i].start()

    for i, j in ((1, t3), (0, t1)):
        r.st_m1[i] = expert_part(j).astype(bf16)
        m_core[i].start()
    r.acc_m[1] = expert_part(t2)
    m_core[1].wait_recv()
    m_send(0)
    r.acc_m[0] = expert_part(t)

    def h_copy(h, block, at, peer):
        block = r.got_h.at[block, pl.ds(h * (N // 2), N // 2)]
        return remote(block, block, one_of(at), None, (e, peer))

    h_y = [h_copy(h, t, 6 + 9 * h, t2) for h in range(2)]
    h_core = [h_copy(h, t, 7 + 9 * h, t1) for h in range(2)]
    h_cross = [h_copy(h, t2, 8 + 9 * h, t1) for h in range(2)]
    for h in range(2):
        f_y[h].wait_recv()
        rows = slice(h * (N // 2), (h + 1) * (N // 2))
        gate = r.acc_f[0, rows] + r.got_f2[h, 0].astype(f32)
        up = r.acc_f[1, rows] + r.got_f2[h, 1].astype(f32)
        r.got_h[t, rows] = (jax.nn.silu(gate) * up).astype(bf16)
        h_y[h].start()
        h_core[h].start()
    m_send(1)
    ep_loop(lambda k: ep_copy(r.st_x, r.got_x, sem_x, k).wait_send())
    for h in range(2):
        h_y[h].wait_recv()
        h_cross[h].start()
    for h in range(2):
        h_core[h].wait_recv()
        h_cross[h].wait_recv()
    local["dense_down"].wait()
    dense = dot(r.got_h[0], r.v_dense_down[0:HQ, :])
    for j in range(1, T):
        dense = dense + dot(r.got_h[j], r.v_dense_down[j * HQ : (j + 1) * HQ, :])
    m_core[0].wait_recv()
    for i in range(2):
        cols = slice(i * half, (i + 1) * half)
        m_y[i].wait_recv()
        final = branch * dense[:, cols] + r.acc_m[0, :, cols] + r.got_m1[0, :, cols].astype(f32)
        final = final + r.got_m2[i].astype(f32)
        r.st_g[:, :, cols] = final.astype(bf16).reshape(E, S, half)
    ep_loop(lambda step: ep_copy(r.st_g, r.got_g, sem_g, step).start())
    r.got_g[e] = r.st_g[e]

    ep_loop(lambda k: ep_copy(r.st_k, r.got_k, sem_k, k).wait_recv())
    new_rows = total_of(r.got_k).astype(bf16)
    r.outs[:, DQ:] = new_rows
    def drain(step):
        ep_copy(r.st_a, r.got_a, sem_a, step).wait_send()
        ep_copy(r.st_r, r.got_r, sem_r, step).wait_send()
        ep_copy(r.st_k, r.got_k, sem_k, step).wait_send()
        c_copy(step).wait_send()
        e_copy(step).wait_send()

    ep_loop(drain)

    @pl.when(jnp.logical_not(here))
    def _():
        c_copy(0).wait_send()


    def drain_all(step):
        src = peer_of(step)
        pass_on(src, t, sem_ey, t2).wait_send()
        pass_on(src, t, sem_ec, t1).wait_send()
        pass_on(src, t2, sem_ez, t1).wait_send()

    all_loop(drain_all)
    for copy in (
        wo_y, wo_core, wo_cross, *dense_swap, *f_y, *m_core, *m_y, *h_y, *h_core, *h_cross
    ):
        copy.wait_send()

    ep_loop(lambda step: ep_copy(r.st_g, r.got_g, sem_g, step).wait())
    total = total_of(r.got_g)
    for k in range(GT):
        at = slice(k * OC, (k + 1) * OC)
        resid = r.got_e[t * GT + k, e].astype(f32)
        r.outs[:, at] = (resid + total[:, at]).astype(bf16)


def body(*args):
    E, T = lax.axis_size("ep"), lax.axis_size("tp")
    given = dict(zip(INPUTS, args))
    S, D = given["tokens"].shape
    N = E * S
    FE, QC = given["query_weight"].shape
    KC = given["key_weight"].shape[1]
    CL, HD = given["cache_keys"].shape[2:]
    G = QC // HD
    OC = given["out_weight"].shape[1]
    GT, DQ = E // T, D // T
    HQ = given["dense_gate"].shape[1] // T
    L = given["expert_gate"].shape[0]
    for name in ("attn_gain", "ffn_gain"):
        given[name] = given[name].reshape(1, D)
    given["branch_gate"] = given["branch_gate"].reshape(D // 128, 128)
    for name in ("route_ids", "route_weights"):
        given[name] = given[name].T

    scratch = {}
    for name in STREAMED:
        if name in SCALARS:
            scratch["v_" + name] = pltpu.SMEM(given[name].shape, given[name].dtype)
        elif name != "out_weight":
            scratch["v_" + name] = pltpu.VMEM(given[name].shape, given[name].dtype)
    scratch["wo_all"] = pltpu.VMEM((T, QC, OC), bf16)
    for name in ("dense_gate", "dense_up"):
        scratch["o_" + name] = pltpu.VMEM(given[name].shape, bf16)

    def pair(name, shape, dtype=bf16):
        scratch["st_" + name] = pltpu.VMEM(shape, dtype)
        scratch["got_" + name] = pltpu.VMEM(shape, dtype)

    pair("a", (E, S, FE))
    pair("r", (E, S, FE))
    pair("q", (E, S, QC))
    pair("k", (E, S, 2 * KC))
    pair("x", (E, L, S, 128), f32)
    scratch["st_c"] = pltpu.VMEM((S, QC), bf16)
    scratch["got_c"] = pltpu.VMEM((T, GT, S, QC), bf16)
    scratch["st_e"] = pltpu.VMEM((GT, S, OC), bf16)
    scratch["got_e"] = pltpu.VMEM((E, E, S, OC), bf16)
    pair("f2", (2, 2, N // 2, HQ))
    pair("m1", (2, N, DQ))
    pair("m2", (2, N, DQ // 2))
    scratch["gate_row"] = pltpu.VMEM((1, D), f32)
    scratch["got_h"] = pltpu.VMEM((T, N, HQ), bf16)
    scratch["got_g"] = pltpu.VMEM((E, S, DQ), bf16)
    if DQ != QC:
        scratch["st_g"] = pltpu.VMEM((E, S, DQ), bf16)
    scratch["q_rows"] = pltpu.VMEM((S * G, HD), f32)
    scratch["mixed_rows"] = pltpu.VMEM((S * G, HD), f32)
    scratch["scores"] = pltpu.VMEM((S * G, CL), f32)
    scratch["normed2"] = pltpu.VMEM((N, D), bf16)
    scratch["acc_f"] = pltpu.VMEM((2, N, HQ), f32)
    scratch["acc_m"] = pltpu.VMEM((2, N, DQ), f32)
    if HQ % 128:
        scratch["all_f"] = pltpu.VMEM((T, 2, N, HQ), f32)

    def sems(name, count):
        scratch[name + "_send"] = pltpu.SemaphoreType.DMA((count,))
        scratch[name + "_recv"] = pltpu.SemaphoreType.DMA((count,))

    for name in ("a", "q", "k", "r", "x", "e", "g"):
        sems(name, E - 1)
    for name in ("c", "ey", "ec", "ez"):
        sems(name, E)
    sems("one", 18)
    scratch["load_sem"] = pltpu.SemaphoreType.DMA((len(STREAMED),))

    in_specs = [pl.BlockSpec(memory_space=pltpu.HBM)] * len(INPUTS)
    names = INPUTS + ("outs",) + tuple(scratch)
    packed = pl.pallas_call(
        functools.partial(layer_kernel, names),
        out_shape=jax.ShapeDtypeStruct((S, DQ + 2 * KC), bf16),
        in_specs=in_specs,
        out_specs=pl.BlockSpec(memory_space=pltpu.VMEM),
        scratch_shapes=list(scratch.values()),
        compiler_params=pltpu.CompilerParams(
            collective_id=0, has_side_effects=True, vmem_limit_bytes=67_043_328
        ),
        name="layer",
    )(*(given[name] for name in INPUTS))

    def part(packed_ref, layer_ref, keys_ref, values_ref):
        layer_ref[...] = packed_ref[:, :DQ]
        keys_ref[...] = packed_ref[:, DQ : DQ + KC]
        values_ref[...] = packed_ref[:, DQ + KC :]

    return pl.pallas_call(
        part,
        out_shape=tuple(jax.ShapeDtypeStruct((S, width), bf16) for width in (DQ, KC, KC)),
        in_specs=[pl.BlockSpec(memory_space=pltpu.VMEM)],
        out_specs=(pl.BlockSpec(memory_space=pltpu.VMEM),) * 3,
        name="part",
    )(packed)


def solution(mesh):
    in_specs = (
        P("ep", None),
        P(),
        P("ep", "tp"),
        P("ep", "tp"),
        P("ep", "tp"),
        P("tp"),
        P("ep", "tp", None, None),
        P("ep", "tp", None, None),
        P("ep"),
        P("tp", "ep"),
        P(),
        P(),
        P("tp", "ep"),
        P("tp", "ep"),
        P("ep", "tp"),
        P("ep", None),
        P("ep", None),
        P("ep", None, "tp"),
        P("ep", None, "tp"),
        P("ep", "tp", None),
    )
    out_specs = (P("ep", "tp"), P("ep", "tp"), P("ep", "tp"))
    return jax.shard_map(body, mesh=mesh, in_specs=in_specs, out_specs=out_specs, check_vma=False)
```

```python
import functools
import jax
import jax.numpy as jnp
from jax import lax
from jax.experimental import pallas as pl
from jax.experimental.pallas import tpu as pltpu
from jax.sharding import PartitionSpec as P

norm_eps = 1e-05
clamp_limit = 7.0
swish_alpha = 1.702
f32, bf16 = jnp.float32, jnp.bfloat16
MESH = pl.DeviceIdType.MESH

INPUTS = (
    "tokens", "attn_gain", "query_weight", "key_weight", "value_weight", "break_bias",
    "cache_keys", "cache_values", "lengths", "out_weight", "ffn_gain", "branch_gate",
    "dense_gate", "dense_up", "dense_down", "route_ids", "route_weights", "expert_gate",
    "expert_up", "expert_down",
)
FIRST = ("tokens", "attn_gain", "query_weight", "out_weight")
SCALARS = ("break_bias", "lengths")
LATER = (
    "route_ids", "route_weights", "branch_gate", "ffn_gain", "key_weight", "value_weight",
    "cache_keys", "dense_gate", "dense_up", "cache_values", "expert_gate", "expert_up",
    "expert_down", "dense_down",
)
STREAMED = FIRST + SCALARS + LATER


def dot(a, b):
    return jnp.dot(a, b, preferred_element_type=f32)


class Refs:
    pass


def layer_kernel(names, *refs):
    r = Refs()
    for name, ref in zip(names, refs):
        setattr(r, name, ref)
    E, T = lax.axis_size("ep"), lax.axis_size("tp")
    e, t = lax.axis_index("ep"), lax.axis_index("tp")
    S, D = r.tokens.shape
    N = E * S
    bits = [1 << i for i in range((E - 1).bit_length())]
    FE = r.query_weight.shape[0]
    QC = r.query_weight.shape[1]
    KC = r.key_weight.shape[1]
    CL, HD = r.cache_keys.shape[2], r.cache_keys.shape[3]
    G = QC // HD
    OC = r.out_weight.shape[1]
    GT = E // T
    DQ = D // T
    HQ = r.dense_gate.shape[1] // T
    L = r.expert_gate.shape[0]
    t1 = t + 1 - 2 * lax.rem(t, 2)
    t2 = lax.rem(t + 2, T)
    t3 = lax.rem(t1 + 2, T)

    local = {}
    caches = {"cache_keys": [], "cache_values": []}
    for i, name in enumerate(STREAMED):
        into = r.wo_all.at[t] if name == "out_weight" else getattr(r, "v_" + name)
        if name in caches:
            sets = into.shape[0]
            for j in range(into.shape[2] // HD):
                block = getattr(r, name).at[pl.ds(j * sets, sets), 0]
                there = into.at[:, :, pl.ds(j * HD, HD)]
                caches[name].append(pltpu.make_async_copy(block, there, r.cache_sem.at[i, j]))
            continue
        local[name] = pltpu.make_async_copy(getattr(r, name), into, r.load_sem.at[i])
    for name in FIRST:
        local[name].start()

    def peer_of(k):
        out = 0
        for bit in bits:
            out = out + bit * lax.rem(lax.rem(e // bit, 2) + (k // bit) % 2, 2)
        return out

    def ep_loop(fn):
        if E <= 8:
            for k in range(E - 1, 0, -1):
                fn(k)
        else:
            lax.fori_loop(1, E, lambda i, carry: (fn(E - i), carry)[1], 0)

    def all_loop(fn):
        fn(0)
        ep_loop(fn)

    barrier = pltpu.get_barrier_semaphore()

    def greet(where):
        pl.semaphore_signal(barrier, inc=1, device_id=where, device_id_type=MESH)

    ep_loop(lambda k: greet((peer_of(k), t)))
    for step in range(1, T):
        greet((e, lax.rem(t + step, T)))

    owner = e // GT
    here = owner == t

    def group_loop(fn):
        def one(i, carry):
            fn(lax.rem(i, T), i // T)
            return carry

        lax.fori_loop(0, E, one, 0)

    def greet_group(source_t, j):
        group = t * GT + j

        @pl.when(jnp.logical_or(group != e, source_t != t))
        def _():
            greet((group, source_t))

    group_loop(greet_group)

    def remote(src, dst, sems, at, where):
        send, recv = sems
        return pltpu.make_async_remote_copy(
            src_ref=src,
            dst_ref=dst,
            send_sem=send if at is None else send.at[at],
            recv_sem=recv if at is None else recv.at[at],
            device_id=where,
            device_id_type=MESH,
        )

    def ep_copy(src, dst, sems, k, per_peer=True):
        peer = peer_of(k)
        return remote(src.at[peer] if per_peer else src, dst.at[e], sems, k - 1, (peer, t))

    sem_a = (r.a_send, r.a_recv)
    sem_q = (r.q_send, r.q_recv)
    sem_k = (r.k_send, r.k_recv)
    sem_r = (r.r_send, r.r_recv)
    sem_x = (r.x_send, r.x_recv)
    sem_e = (r.e_send, r.e_recv)
    sem_ey = (r.ey_send, r.ey_recv)
    sem_ec = (r.ec_send, r.ec_recv)
    sem_ez = (r.ez_send, r.ez_recv)
    sem_g = (r.g_send, r.g_recv)

    def one_of(at):
        return (r.one_send.at[at], r.one_recv.at[at])

    local["tokens"].wait()
    local["attn_gain"].wait()
    tokens = r.v_tokens[...].astype(f32)
    mean = jnp.mean(tokens * tokens, axis=-1, keepdims=True)
    normed = (tokens * lax.rsqrt(mean + norm_eps) * r.v_attn_gain[...]).astype(bf16)
    for p in range(E):
        r.st_a[p] = normed[:, p * FE : (p + 1) * FE]
    pl.semaphore_wait(barrier, E - 1 + T - 1 + E - jnp.where(here, 1, 0))

    ep_loop(lambda step: ep_copy(r.st_a, r.got_a, sem_a, step).start())
    for name in SCALARS + LATER:
        for copy in caches.get(name) or [local[name]]:
            copy.start()
    r.got_a[e] = r.st_a[e]
    for p in range(E):
        r.st_r[p] = r.v_tokens[:, p * FE : (p + 1) * FE]
    r.got_r[e] = r.st_r[e]
    def wo_copy(block, at, peer):
        block = r.wo_all.at[block]
        return remote(block, block, one_of(at), None, (e, peer))

    wo_y, wo_core, wo_cross = wo_copy(t, 0, t2), wo_copy(t, 1, t1), wo_copy(t2, 3, t1)
    local["out_weight"].wait()
    wo_y.start()
    wo_core.start()
    local["query_weight"].wait()
    r.got_q[e] = dot(r.st_a[e], r.v_query_weight[...]).astype(bf16)

    def answered(k):
        src = peer_of(k)
        return remote(r.st_q.at[src], r.got_q.at[e], sem_q, k - 1, (src, t))

    def answer(k):
        ep_copy(r.st_a, r.got_a, sem_a, k).wait_recv()
        src = peer_of(k)
        r.st_q[src] = dot(r.got_a[src], r.v_query_weight[...]).astype(bf16)
        answered(k).start()

    ep_loop(answer)
    local["key_weight"].wait()
    local["value_weight"].wait()
    rows = r.got_a[...].reshape(N, FE)
    r.st_k[:, :, :KC] = dot(rows, r.v_key_weight[...]).astype(bf16).reshape(E, S, KC)
    r.st_k[:, :, KC:] = dot(rows, r.v_value_weight[...]).astype(bf16).reshape(E, S, KC)
    r.got_k[e] = r.st_k[e]
    diagonal = lax.broadcasted_iota(jnp.int32, (S, S), 0)
    diagonal = diagonal == lax.broadcasted_iota(jnp.int32, (S, S), 1)

    def column(line):
        spread = jnp.broadcast_to(line, (S, S))
        return jnp.sum(jnp.where(diagonal, spread, 0.0), axis=1, keepdims=True)

    for name in ("route_ids", "route_weights", "branch_gate", "ffn_gain"):
        local[name].wait()
    picks = r.route_ids.shape[0]
    ids = [column(r.v_route_ids[k : k + 1, :].astype(f32)) for k in range(picks)]
    route = [column(r.v_route_weights[k : k + 1, :]) for k in range(picks)]

    first_lanes = lax.broadcasted_iota(jnp.int32, (S, 128), 1) < 64

    def side(p, carry):
        for l in range(L):
            expert = jnp.full((S, 1), p * L + l, jnp.int32).astype(f32)
            own = jnp.zeros((S, 1), f32)
            for k in range(picks):
                own = own + jnp.where(ids[k] == expert, route[k], 0.0)
            wide = jnp.broadcast_to(own, (S, 128))
            high = wide.astype(bf16)
            low_part = (wide - high.astype(f32)).astype(bf16)
            r.st_x[p, l] = jnp.where(first_lanes, high, low_part)
        return carry

    lax.fori_loop(0, E, side, 0)
    r.got_x[e] = r.st_x[e]
    for p in range(D // 128):
        r.gate_row[:, p * 128 : (p + 1) * 128] = r.v_branch_gate[p : p + 1, :].astype(f32)

    dense_swap = [
        remote(r.v_dense_gate, r.o_dense_gate, one_of(4), None, (e, t1)),
        remote(r.v_dense_up, r.o_dense_up, one_of(5), None, (e, t1)),
    ]
    for name in ("dense_gate", "dense_up"):
        local[name].wait()
    for copy in dense_swap:
        copy.start()

    def r_copy(k):
        peer = peer_of(k)
        return pltpu.make_async_remote_copy(
            src_ref=r.st_r.at[peer],
            dst_ref=r.got_r.at[e],
            send_sem=r.r_send.at[peer],
            recv_sem=r.r_recv.at[e],
            device_id=(peer, t),
            device_id_type=MESH,
        )

    ep_loop(lambda k: answered(k).wait_recv())
    @pl.when(here)
    def _():
        ep_loop(lambda k: r_copy(k).start())

    ep_loop(lambda k: ep_copy(r.st_x, r.got_x, sem_x, k).start())
    wo_y.wait_recv()
    wo_cross.start()
    def total_of(got):
        def add(j, total):
            return total + got[j].astype(f32)

        return lax.fori_loop(1, E, add, got[0].astype(f32))

    queries = total_of(r.got_q).astype(bf16).astype(f32)
    tile = 8
    per = tile // G
    sets = S // per
    low = lax.broadcasted_iota(jnp.int32, (tile, 1), 0)
    for j in range(per):
        for h in range(G):
            block = queries[j * sets : (j + 1) * sets, h * HD : (h + 1) * HD]
            r.q_rows[pl.ds(j * G + h, sets, stride=tile), :] = block

    def spread(x):
        parts = [jnp.where(low // G == j, x, 0.0) for j in range(per)]
        return jnp.concatenate(parts, axis=1)

    def pick(x):
        out = x[:, :HD]
        for j in range(1, per):
            out = jnp.where(low // G == j, x[:, j * HD : (j + 1) * HD], out)
        return out

    for copy in caches["cache_keys"]:
        copy.wait()
    for i in range(sets):
        q8 = spread(r.q_rows[i * tile : (i + 1) * tile, :]).astype(bf16)
        r.scores[i * tile : (i + 1) * tile, :] = lax.dot_general(
            q8, r.v_cache_keys[i], (((1,), (1,)), ((), ())), preferred_element_type=f32
        )
    for name in SCALARS:
        local[name].wait()
    heads = S * G
    row = lax.broadcasted_iota(jnp.int32, (heads, 1), 0)
    length = jnp.zeros((heads, 1), jnp.int32)
    bias = jnp.zeros((heads, 1), f32)
    for s in range(S):
        at = (s % sets) * per + s // sets
        length = jnp.where(row // G == at, r.v_lengths[s], length)
    for h in range(G):
        bias = jnp.where(lax.rem(row, G) == h, r.v_break_bias[h], bias)
    W = min(256, CL)
    later = lax.broadcasted_iota(jnp.int32, (W, W), 0)
    later = later > lax.broadcasted_iota(jnp.int32, (W, W), 1)
    later = jnp.where(later, 1.0, 0.0).astype(bf16)
    after = jnp.zeros((heads, 1), f32)
    for c in reversed(range(CL // W)):
        z = r.scores[:, c * W : (c + 1) * W] * HD ** (-0.5) + bias
        inside = lax.broadcasted_iota(jnp.int32, (heads, W), 1) + c * W < length
        soft = jnp.log1p(jnp.exp(-jnp.abs(z)))
        keep = jnp.where(inside, -(jnp.maximum(z, 0.0) + soft), 0.0)
        high = keep.astype(bf16)
        rest = keep - high.astype(f32)
        middle = rest.astype(bf16)
        least = (rest - middle.astype(f32)).astype(bf16)
        between = dot(high, later) + dot(middle, later) + dot(least, later) + after
        after = after + jnp.sum(keep, axis=1, keepdims=True)
        chance = jnp.exp(jnp.minimum(z, 0.0) - soft + between)
        r.scores[:, c * W : (c + 1) * W] = jnp.where(inside, chance, 0.0)
    for copy in caches["cache_values"]:
        copy.wait()
    for i in range(sets):
        w8 = r.scores[i * tile : (i + 1) * tile, :].astype(bf16)
        r.mixed_rows[i * tile : (i + 1) * tile, :] = pick(dot(w8, r.v_cache_values[i]))
    for h in range(G):
        parts = [r.mixed_rows[pl.ds(j * G + h, sets, stride=tile), :] for j in range(per)]
        r.st_c[:, h * HD : (h + 1) * HD] = jnp.concatenate(parts, axis=0).astype(bf16)
    def c_copy(k):
        peer = peer_of(k)
        block = r.got_c.at[t, lax.rem(e, GT)]
        return pltpu.make_async_remote_copy(
            src_ref=r.st_c,
            dst_ref=block,
            send_sem=r.c_send.at[k],
            recv_sem=r.c_recv.at[t * GT + lax.rem(e, GT)],
            device_id=(peer, owner),
            device_id_type=MESH,
        )

    def c_arrival(source_t, j):
        return pltpu.make_async_remote_copy(
            src_ref=r.st_c,
            dst_ref=r.got_c.at[source_t, j],
            send_sem=r.c_send.at[0],
            recv_sem=r.c_recv.at[source_t * GT + j],
            device_id=(t * GT + j, source_t),
            device_id_type=MESH,
        )

    ep_loop(lambda k: c_copy(k).start())

    @pl.when(jnp.logical_not(here))
    def _():
        c_copy(0).start()

    @pl.when(here)
    def _():
        r.got_c[t, lax.rem(e, GT)] = r.st_c[...]


    def r_wait(j, carry):
        group = t * GT + j

        @pl.when(group != e)
        def _():
            remote(r.st_r.at[e], r.got_r.at[group], sem_r, group, (group, t)).wait_recv()

        return carry

    lax.fori_loop(0, GT, r_wait, 0)
    ep_loop(lambda k: answered(k).wait_send())
    if DQ == QC:
        r.st_g = r.st_q
    wo_core.wait_recv()
    wo_cross.wait_recv()

    def c_wait(source_t, j):
        @pl.when(jnp.logical_or(t * GT + j != e, source_t != t))
        def _():
            c_arrival(source_t, j).wait_recv()

    group_loop(c_wait)
    mixed = dot(r.got_c[0].reshape(GT * S, QC), r.wo_all[0])
    for j in range(1, T):
        mixed = mixed + dot(r.got_c[j].reshape(GT * S, QC), r.wo_all[j])
    mixed = mixed.astype(bf16).astype(f32).reshape(GT, S, OC)

    mine = pl.ds(t * GT, GT)
    r.st_e[...] = (r.got_r[mine].astype(f32) + mixed).astype(bf16)

    def e_copy(k):
        return remote(r.st_e, r.got_e.at[e, mine], sem_e, k - 1, (peer_of(k), t))

    ep_loop(lambda step: e_copy(step).start())
    r.got_e[e, mine] = r.st_e[...]

    def pass_on(src, group, sems, peer):
        block = r.got_e.at[src, pl.ds(group * GT, GT)]
        return remote(block, block, sems, src, (e, peer))

    remote(r.st_e, r.got_e.at[e, mine], sem_ey, e, (e, t2)).start()
    remote(r.st_e, r.got_e.at[e, mine], sem_ec, e, (e, t1)).start()

    def forward(step):
        e_copy(step).wait_recv()
        src = peer_of(step)
        pass_on(src, t, sem_ey, t2).start()
        pass_on(src, t, sem_ec, t1).start()

    ep_loop(forward)

    def cross(step):
        src = peer_of(step)
        pass_on(src, t, sem_ey, t2).wait_recv()
        pass_on(src, t2, sem_ez, t1).start()

    HN = N // 2
    plane = t // 2
    starts = (plane * HN, (1 - plane) * HN)
    pairs = ((r.v_dense_gate, r.o_dense_gate), (r.v_dense_up, r.o_dense_up))
    f_y = [remote(r.st_f2.at[h], r.got_f2.at[h], one_of((2, 13)[h]), None, (e, t2)) for h in range(2)]

    def half_of(h):
        groups = pl.ds((plane if h == 0 else 1 - plane) * (E // 2), E // 2)
        rows = pl.ds(pl.multiple_of(starts[h], HN), HN)
        squares = jnp.zeros((HN, OC), f32)
        for p in range(E):
            x = r.got_e[p, groups].reshape(HN, OC).astype(f32)
            squares = squares + x * x
        inverse = lax.rsqrt(jnp.sum(squares, axis=1, keepdims=True) * (1.0 / D) + norm_eps)
        gate_sum = jnp.zeros((HN, OC), f32)
        for p in range(E):
            at = slice(p * OC, (p + 1) * OC)
            x = r.got_e[p, groups].reshape(HN, OC).astype(f32)
            x = (x * inverse * r.v_ffn_gain[:, at]).astype(bf16)
            r.normed2[rows, at] = x
            gate_sum = gate_sum + x.astype(f32) * r.gate_row[:, at]
        branch = jax.nn.sigmoid(jnp.sum(gate_sum, axis=1, keepdims=True))
        r.branch[rows, :] = jnp.broadcast_to(branch, (HN, 128))
        own = r.normed2[rows, pl.ds(pl.multiple_of(t * DQ, 128), DQ)]
        other = r.normed2[rows, pl.ds(pl.multiple_of(t1 * DQ, 128), DQ)]
        whole_lanes = HQ % 128 == 0
        if not whole_lanes:
            for j in range(T):
                cols = slice(j * HQ, (j + 1) * HQ)
                for k in range(2):
                    part = dot(own, pairs[k][0][:, cols]) + dot(other, pairs[k][1][:, cols])
                    r.all_f[j, k] = part

        def dense_part(j, k):
            if not whole_lanes:
                return r.all_f[j, k]
            cols = pl.ds(pl.multiple_of(j * HQ, 128), HQ)
            return dot(own, pairs[k][0][:, cols]) + dot(other, pairs[k][1][:, cols])

        for k in range(2):
            r.st_f2[h, k] = dense_part(t2, k).astype(bf16)
        f_y[h].start()
        if not whole_lanes:
            for k in range(2):
                r.acc_f[k, rows] = dense_part(t, k)

    cross(0)
    if E <= 8:
        for k in range(E - 1, 2, -1):
            cross(k)

    def landed_core(step):
        pass_on(peer_of(step), t, sem_ec, t1).wait_recv()

    all_loop(landed_core)
    for copy in dense_swap:
        copy.wait_recv()
    half_of(0)
    if E <= 8:
        for k in range(2, 0, -1):
            cross(k)
    else:
        ep_loop(cross)

    def landed(step):
        pass_on(peer_of(step), t2, sem_ez, t1).wait_recv()

    all_loop(landed)
    half_of(1)
    if HQ % 128 == 0:
        own = r.normed2[:, pl.ds(pl.multiple_of(t * DQ, 128), DQ)]
        other = r.normed2[:, pl.ds(pl.multiple_of(t1 * DQ, 128), DQ)]
        cols = pl.ds(pl.multiple_of(t * HQ, 128), HQ)
        for k in range(2):
            r.acc_f[k] = dot(own, pairs[k][0][:, cols]) + dot(other, pairs[k][1][:, cols])
    ep_loop(lambda k: ep_copy(r.st_k, r.got_k, sem_k, k).start())

    rows = r.normed2[...]
    local["expert_gate"].wait()
    local["expert_up"].wait()
    local["expert_down"].wait()
    units = []
    for l in range(L):
        gate = jnp.minimum(dot(rows, r.v_expert_gate[l]), clamp_limit)
        up = jnp.clip(dot(rows, r.v_expert_up[l]), -clamp_limit, clamp_limit)
        units.append(((up + 1.0) * gate * jax.nn.sigmoid(swish_alpha * gate)).astype(bf16))

    def h_copy(block, start, at, peer):
        block = r.got_h.at[block, pl.ds(pl.multiple_of(start, HN), HN)]
        return remote(block, block, one_of(at), None, (e, peer))

    h_y = [h_copy(t, starts[1 - h], 6 + 9 * h, t2) for h in range(2)]
    h_core = [h_copy(t, starts[1 - h], 7 + 9 * h, t1) for h in range(2)]
    h_cross = [h_copy(t2, starts[h], 8 + 9 * h, t1) for h in range(2)]

    def finish_half(h):
        f_y[h].wait_recv()
        rows = pl.ds(pl.multiple_of(starts[1 - h], HN), HN)
        gate = r.acc_f[0, rows] + r.got_f2[h, 0].astype(f32)
        up = r.acc_f[1, rows] + r.got_f2[h, 1].astype(f32)
        r.got_h[t, rows] = (jax.nn.silu(gate) * up).astype(bf16)
        h_y[h].start()
        h_core[h].start()

    ep_loop(lambda k: ep_copy(r.st_x, r.got_x, sem_x, k).wait_recv())

    def expert_part(j):
        out = None
        for l in range(L):
            pieces = r.got_x[:, l].reshape(N, 128).astype(f32)
            scale = pieces[:, :1] + pieces[:, 64:65]
            cols = pl.ds(pl.multiple_of(j * DQ, 128), DQ)
            one = scale * dot(units[l], r.v_expert_down[l, :, cols])
            out = one if out is None else out + one
        return out

    m_core = [remote(r.st_m1.at[i], r.got_m1.at[i], one_of(11 + i), None, (e, t1)) for i in range(2)]
    half = DQ // 2
    m_y = [remote(r.st_m2.at[i], r.got_m2.at[i], one_of(9 + i), None, (e, t2)) for i in range(2)]

    def m_send(i):
        cols = slice(i * half, (i + 1) * half)
        r.st_m2[i] = (r.acc_m[1, :, cols] + r.got_m1[1, :, cols].astype(f32)).astype(bf16)
        m_y[i].start()

    for i, j in ((1, t3), (0, t1)):
        r.st_m1[i] = expert_part(j).astype(bf16)
        m_core[i].start()
    r.acc_m[1] = expert_part(t2)
    m_core[1].wait_recv()
    m_send(0)
    r.acc_m[0] = expert_part(t)

    finish_half(0)
    finish_half(1)
    m_send(1)
    ep_loop(lambda k: ep_copy(r.st_x, r.got_x, sem_x, k).wait_send())
    for h in range(2):
        h_y[h].wait_recv()
        h_cross[h].start()
    for h in range(2):
        h_core[h].wait_recv()
        h_cross[h].wait_recv()
    local["dense_down"].wait()
    dense = dot(r.got_h[0], r.v_dense_down[0:HQ, :])
    for j in range(1, T):
        dense = dense + dot(r.got_h[j], r.v_dense_down[j * HQ : (j + 1) * HQ, :])
    m_core[0].wait_recv()
    for i in range(2):
        cols = slice(i * half, (i + 1) * half)
        m_y[i].wait_recv()
        final = r.branch[:, :1] * dense[:, cols] + r.acc_m[0, :, cols] + r.got_m1[0, :, cols].astype(f32)
        final = final + r.got_m2[i].astype(f32)
        r.st_g[:, :, cols] = final.astype(bf16).reshape(E, S, half)
    ep_loop(lambda step: ep_copy(r.st_g, r.got_g, sem_g, step).start())
    r.got_g[e] = r.st_g[e]

    ep_loop(lambda k: ep_copy(r.st_k, r.got_k, sem_k, k).wait_recv())
    new_rows = total_of(r.got_k).astype(bf16)
    r.outs[:, DQ:] = new_rows
    def drain(step):
        ep_copy(r.st_a, r.got_a, sem_a, step).wait_send()
        ep_copy(r.st_k, r.got_k, sem_k, step).wait_send()
        c_copy(step).wait_send()
        e_copy(step).wait_send()

    ep_loop(drain)

    @pl.when(here)
    def _():
        ep_loop(lambda k: r_copy(k).wait_send())

    @pl.when(jnp.logical_not(here))
    def _():
        c_copy(0).wait_send()


    def drain_all(step):
        src = peer_of(step)
        pass_on(src, t, sem_ey, t2).wait_send()
        pass_on(src, t, sem_ec, t1).wait_send()
        pass_on(src, t2, sem_ez, t1).wait_send()

    all_loop(drain_all)
    for copy in (
        wo_y, wo_core, wo_cross, *dense_swap, *f_y, *m_core, *m_y, *h_y, *h_core, *h_cross
    ):
        copy.wait_send()

    ep_loop(lambda step: ep_copy(r.st_g, r.got_g, sem_g, step).wait())
    total = total_of(r.got_g)
    for k in range(GT):
        at = slice(k * OC, (k + 1) * OC)
        resid = r.got_e[t * GT + k, e].astype(f32)
        r.outs[:, at] = (resid + total[:, at]).astype(bf16)


def body(*args):
    E, T = lax.axis_size("ep"), lax.axis_size("tp")
    given = dict(zip(INPUTS, args))
    S, D = given["tokens"].shape
    N = E * S
    FE, QC = given["query_weight"].shape
    KC = given["key_weight"].shape[1]
    CL, HD = given["cache_keys"].shape[2:]
    G = QC // HD
    OC = given["out_weight"].shape[1]
    GT, DQ = E // T, D // T
    HQ = given["dense_gate"].shape[1] // T
    L = given["expert_gate"].shape[0]
    for name in ("attn_gain", "ffn_gain"):
        given[name] = given[name].reshape(1, D)
    given["branch_gate"] = given["branch_gate"].reshape(D // 128, 128)
    for name in ("route_ids", "route_weights"):
        given[name] = given[name].T

    scratch = {}
    for name in STREAMED:
        if name in SCALARS:
            scratch["v_" + name] = pltpu.SMEM(given[name].shape, given[name].dtype)
        elif name in ("cache_keys", "cache_values"):
            per = 8 // G
            scratch["v_" + name] = pltpu.VMEM((S // per, CL, per * HD), bf16)
        elif name != "out_weight":
            scratch["v_" + name] = pltpu.VMEM(given[name].shape, given[name].dtype)
    scratch["wo_all"] = pltpu.VMEM((T, QC, OC), bf16)
    for name in ("dense_gate", "dense_up"):
        scratch["o_" + name] = pltpu.VMEM(given[name].shape, bf16)

    def pair(name, shape, dtype=bf16):
        scratch["st_" + name] = pltpu.VMEM(shape, dtype)
        scratch["got_" + name] = pltpu.VMEM(shape, dtype)

    pair("a", (E, S, FE))
    pair("r", (E, S, FE))
    pair("q", (E, S, QC))
    pair("k", (E, S, 2 * KC))
    pair("x", (E, L, S, 128))
    scratch["st_c"] = pltpu.VMEM((S, QC), bf16)
    scratch["got_c"] = pltpu.VMEM((T, GT, S, QC), bf16)
    scratch["st_e"] = pltpu.VMEM((GT, S, OC), bf16)
    scratch["got_e"] = pltpu.VMEM((E, E, S, OC), bf16)
    pair("f2", (2, 2, N // 2, HQ))
    pair("m1", (2, N, DQ))
    pair("m2", (2, N, DQ // 2))
    scratch["gate_row"] = pltpu.VMEM((1, D), f32)
    scratch["got_h"] = pltpu.VMEM((T, N, HQ), bf16)
    scratch["got_g"] = pltpu.VMEM((E, S, DQ), bf16)
    if DQ != QC:
        scratch["st_g"] = pltpu.VMEM((E, S, DQ), bf16)
    scratch["q_rows"] = pltpu.VMEM((S * G, HD), f32)
    scratch["mixed_rows"] = pltpu.VMEM((S * G, HD), f32)
    scratch["scores"] = pltpu.VMEM((S * G, CL), f32)
    scratch["normed2"] = pltpu.VMEM((N, D), bf16)
    scratch["acc_f"] = pltpu.VMEM((2, N, HQ), f32)
    scratch["branch"] = pltpu.VMEM((N, 128), f32)
    scratch["acc_m"] = pltpu.VMEM((2, N, DQ), f32)
    if HQ % 128:
        scratch["all_f"] = pltpu.VMEM((T, 2, N // 2, HQ), f32)

    def sems(name, count):
        scratch[name + "_send"] = pltpu.SemaphoreType.DMA((count,))
        scratch[name + "_recv"] = pltpu.SemaphoreType.DMA((count,))

    for name in ("a", "q", "k", "x", "e", "g"):
        sems(name, E - 1)
    for name in ("r", "c", "ey", "ec", "ez"):
        sems(name, E)
    sems("one", 18)
    scratch["cache_sem"] = pltpu.SemaphoreType.DMA((len(STREAMED), 8 // G))
    scratch["load_sem"] = pltpu.SemaphoreType.DMA((len(STREAMED),))

    in_specs = [pl.BlockSpec(memory_space=pltpu.HBM)] * len(INPUTS)
    names = INPUTS + ("outs",) + tuple(scratch)
    packed = pl.pallas_call(
        functools.partial(layer_kernel, names),
        out_shape=jax.ShapeDtypeStruct((S, DQ + 2 * KC), bf16),
        in_specs=in_specs,
        out_specs=pl.BlockSpec(memory_space=pltpu.VMEM),
        scratch_shapes=list(scratch.values()),
        compiler_params=pltpu.CompilerParams(
            collective_id=0, has_side_effects=True, vmem_limit_bytes=67_043_328
        ),
        name="layer",
    )(*(given[name] for name in INPUTS))

    def part(packed_ref, layer_ref, keys_ref, values_ref):
        layer_ref[...] = packed_ref[:, :DQ]
        keys_ref[...] = packed_ref[:, DQ : DQ + KC]
        values_ref[...] = packed_ref[:, DQ + KC :]

    return pl.pallas_call(
        part,
        out_shape=tuple(jax.ShapeDtypeStruct((S, width), bf16) for width in (DQ, KC, KC)),
        in_specs=[pl.BlockSpec(memory_space=pltpu.VMEM)],
        out_specs=(pl.BlockSpec(memory_space=pltpu.VMEM),) * 3,
        name="part",
    )(packed)


def solution(mesh):
    in_specs = (
        P("ep", None),
        P(),
        P("ep", "tp"),
        P("ep", "tp"),
        P("ep", "tp"),
        P("tp"),
        P("ep", "tp", None, None),
        P("ep", "tp", None, None),
        P("ep"),
        P("tp", "ep"),
        P(),
        P(),
        P("tp", "ep"),
        P("tp", "ep"),
        P("ep", "tp"),
        P("ep", None),
        P("ep", None),
        P("ep", None, "tp"),
        P("ep", None, "tp"),
        P("ep", "tp", None),
    )
    out_specs = (P("ep", "tp"), P("ep", "tp"), P("ep", "tp"))
    return jax.shard_map(body, mesh=mesh, in_specs=in_specs, out_specs=out_specs, check_vma=False)
```
